32 devices in a mesh: ep: 16 (over z, y, x), tp: 2 (over core).
Axes of the slice: x: 2, y: 2, z: 4, core: 2. Of those that a mesh axis runs over, the one named last changes fastest.
Arguments:
- tokens: bfloat16 [32, 2048], P('ep'), may hold values from -6 to 6
- head_state: float32 [32, 32, 64, 128], P('ep', 'tp'), may hold values from -4 to 4
- conv_state: bfloat16 [32, 3, 2048], P('ep', None, 'tp'), may hold values from -6 to 6
- conv_proj_state: bfloat16 [32, 3, 2, 512], P('ep', None, None, 'tp'), may hold values from -6 to 6
- first_gain: float32 [2048], replicated, may hold values from 0.1 to 1.9
- gate_weight: bfloat16 [2048, 2048], P('ep', 'tp'), may hold values from -0.125 to 0.125
- inner_weight: bfloat16 [2048, 2048], P('ep', 'tp'), may hold values from -0.125 to 0.125
- write_weight: bfloat16 [2048, 512], P(None, 'tp'), may hold values from -0.125 to 0.125
- read_weight: bfloat16 [2048, 512], P(None, 'tp'), may hold values from -0.125 to 0.125
- step_weight: bfloat16 [2048, 32], P(None, 'tp'), may hold values from -0.125 to 0.125
- conv_kernel: float32 [4, 2048], P(None, 'tp'), may hold values from -3 to 3
- conv_proj_kernel: float32 [4, 2, 512], P(None, None, 'tp'), may hold values from -3 to 3
- step_bias: float32 [32], P('tp'), may hold values from -2 to 1
- log_rate: float32 [32], P('tp'), may hold values from -4.5 to 1.5
- skip_gain: float32 [32], P('tp'), may hold values from 0.5 to 2
- group_gain: float32 [2048], P('tp'), may hold values from 0.1 to 1.9
- out_weight: bfloat16 [2048, 2048], P('tp', 'ep'), may hold values from -0.125 to 0.125
- second_gain: float32 [2048], replicated, may hold values from 0.1 to 1.9
- routes: int32 [32, 4], P('ep'), may hold values from 0 to 15, all different within a row; in each aligned block of 32 rows (0 to 31, 32 to 63, ...) at most 32 rows name the same one
- route_logits: bfloat16 [32, 4], P('ep'), may hold values from -8 to 300
- expert_gate: bfloat16 [16, 2048, 1024], P('ep', None, 'tp'), may hold values from -0.5 to 0.5
- expert_up: bfloat16 [16, 2048, 1024], P('ep', None, 'tp'), may hold values from -0.5 to 0.5
- expert_down: bfloat16 [16, 1024, 2048], P('ep', 'tp'), may hold values from -0.0234375 to 0.0234375
- dense_up: bfloat16 [2048, 4096], P(None, ('ep', 'tp')), may hold values from -0.125 to 0.125
- dense_down: bfloat16 [4096, 2048], P(('ep', 'tp')), may hold values from -0.09375 to 0.09375
- dense_gate: float32 [2048], replicated, may hold values from -0.125 to 0.125
Outputs:
- layer_out: bfloat16 [32, 2048], P(('ep', 'tp'))
- state_out: float32 [32, 32, 64, 128], P('ep', 'tp')
- conv_out: bfloat16 [32, 3, 2048], P('ep', None, 'tp')
- conv_proj_out: bfloat16 [32, 3, 2, 512], P('ep', None, None, 'tp')
The draws below stay inside these ranges and needn't reach their ends.
Inputs may be any that keep to these rules, and one draw needn't show every extreme that they name: `routes`: each token names 4 different experts; over the whole batch no expert is named by more than 32 rows, a bound that some block reaches.
All inputs are finite; a program needn't handle non-finite values.
Results may differ from the reference program's by a relative error of at most 0.015.
Values may be sent and summed in bfloat16 or wider, within the bound.
No kernel may reach another device: no remote copies, remote signals or barrier semaphores. Data moves between devices by JAX's collectives and lax.ppermute only.
A program may use at most 64 MiB of HBM per device.

```python
import math
import jax
import jax.numpy as jnp
import numpy as np
from jax import lax

D = 2048
HEADS = 32
HEAD_DIM = 64
STATE = 128
GROUPS = 4
KCONV = 4
DE = 1024
FD = 4096
TOPK = 4
INNER = 2048
GS = 512
EXPERTS = 16
TOKENS = 32
CAPACITY = 32


def draw_log_rate(key, part):
    return jax.random.uniform(key, (HEADS,), jnp.float32, -3.5, 1.5)


def draw_route_logits(key, part):
    base_key = jax.random.fold_in(key, 11)
    values = jnp.clip(1.5 * jax.random.normal(base_key, (TOKENS, TOPK), jnp.float32), -6.0, 6.0)
    return values.astype(jnp.bfloat16)


def steps_of(key, dims, split, low, high):
    level = 1.0
    for axis_at, parts in split:
        heights = jax.random.uniform(jax.random.fold_in(jax.random.fold_in(key, 6), axis_at), (parts,), jnp.float32, low / len(split), high / len(split))
        level = level * jnp.repeat(jnp.exp(heights), dims[axis_at] // parts).reshape((-1,) + (1,) * (len(dims) - 1 - axis_at))
    return level


def deal_out(stream_key, own, number, rows, amount, top, bound, slope):
    order = jax.random.permutation(stream_key, amount)
    packed, common = shares(amount, rows * top, bound, slope, True), shares(amount, rows * top, bound, slope, False)
    places = jnp.arange(amount)

    def named(sizes, rotation):
        used = int((sizes > 0).sum())
        fixed = max(1, used // 4)
        moved = fixed + (places - fixed + rotation * (used - fixed)) % max(1, amount - fixed)
        return jnp.zeros((amount,), jnp.int32).at[order[jnp.where(places < fixed, places, moved)]].set(jnp.asarray(sizes, jnp.int32))

    sizes = jnp.where(number % 4 == 0, named(packed, number // 4), named(common, number - number // 4 - 1))
    mixed = jax.random.permutation(jax.random.fold_in(own, 3), amount)
    giver, taker = mixed[0:amount // 2 * 2:2], mixed[1:amount // 2 * 2:2]
    room = jnp.minimum(sizes[giver] - 1, bound - sizes[taker]) // 2
    room = jnp.where((giver == order[0]) | (taker == order[0]) | (sizes[taker] == 0), 0, jnp.maximum(room, 0))
    moved = jax.random.randint(jax.random.fold_in(own, 4), (amount // 2,), 0, 1 << 20) % (room + 1)
    sizes = sizes.at[giver].add(-moved).at[taker].add(moved)
    items = jnp.searchsorted(jnp.cumsum(sizes), jnp.arange(rows * top), side="right").astype(jnp.int32)
    grid = items.reshape(top, rows).T
    grid = grid[jax.random.permutation(jax.random.fold_in(own, 1), rows)]
    rotation = jax.random.randint(jax.random.fold_in(own, 2), (rows, 1), 0, top)
    return jnp.take_along_axis(grid, (jnp.arange(top)[None, :] + rotation) % top, axis=1)


def shares(count, total, bound, skew, full):
    weights = [(1 << 20) // math.isqrt(rank ** skew) + 1 for rank in range(1, count + 1)]
    largest = bound if full else min(bound, max(-(-total // count), total * weights[0] // sum(weights)))
    least = 1 if total - largest >= count - 1 else 0
    holding, rest = [largest] + [least] * (count - 1), total - largest - least * (count - 1)
    while rest > 0:
        free = [i for i in range(1, count) if holding[i] < largest] or [i for i in range(1, count) if holding[i] < bound]
        mass, remaining = sum([weights[i] for i in free]), rest
        for i in free:
            addition = min(bound - holding[i], max(1, remaining * weights[i] // mass), rest)
            holding[i] = holding[i] + addition
            rest = rest - addition
    return np.array(holding)


def centred(key, extent, width, limit, cuts=(), kind=jnp.bfloat16):
    array = jax.random.normal(key, extent, jnp.float32) * width
    if len(cuts) > 0:
        array = steps_of(key, extent, cuts, -0.22, 0.18) * array
    return jnp.clip(array, min=-limit, max=limit).astype(kind)


def setup_inputs(seed: int = 0) -> dict:
    streams_of = jax.random.split(jax.random.key(seed), 27)
    tokens = centred(streams_of[0], (TOKENS, D), 1.0, 6.0, ((0, 16),))
    head_state = centred(streams_of[1], (TOKENS, HEADS, HEAD_DIM, STATE), 0.5, 4.0, ((0, 16), (1, 2)), jnp.float32)
    conv_state = centred(streams_of[2], (TOKENS, KCONV - 1, INNER), 1.0, 6.0, ((0, 16), (2, 2)))
    conv_proj_state = centred(streams_of[3], (TOKENS, KCONV - 1, 2, GS), 1.0, 6.0, ((0, 16), (3, 2)))
    first_gain = jnp.clip(1.0 + 0.18 * jax.random.normal(streams_of[4], (D,), jnp.float32), 0.1, 1.9)
    gate_weight = centred(streams_of[5], (D, INNER), D ** -0.5, 0.125, ((0, 16), (1, 2)))
    inner_weight = centred(streams_of[6], (D, INNER), D ** -0.5, 0.125, ((0, 16), (1, 2)))
    write_weight = centred(streams_of[7], (D, GS), D ** -0.5, 0.125, ((1, 2),))
    read_weight = centred(streams_of[8], (D, GS), D ** -0.5, 0.125, ((1, 2),))
    step_weight = centred(streams_of[9], (D, HEADS), D ** -0.5, 0.125, ((1, 2),))
    conv_kernel = centred(streams_of[10], (KCONV, INNER), 0.5, 3.0, ((1, 2),), jnp.float32)
    conv_proj_kernel = centred(streams_of[11], (KCONV, 2, GS), 0.5, 3.0, ((2, 2),), jnp.float32)
    step_bias = jnp.clip(-2.0 + 3.0 * jax.random.uniform(streams_of[12], (HEADS,), jnp.float32) ** steps_of(streams_of[12], (HEADS,), ((0, 2),), -0.2, 0.2), -2.0, 1.0)
    log_rate = draw_log_rate(jax.random.fold_in(streams_of[26], 71), 0)
    skip_gain = jnp.clip(0.5 + 1.5 * jax.random.uniform(streams_of[14], (HEADS,), jnp.float32) ** steps_of(streams_of[14], (HEADS,), ((0, 2),), -0.2, 0.2), 0.5, 2.0)
    group_gain = jnp.clip(1.0 + 0.18 * jax.random.normal(streams_of[15], (INNER,), jnp.float32), 0.1, 1.9)
    out_weight = centred(streams_of[16], (INNER, D), INNER ** -0.5, 0.125, ((0, 2), (1, 16)))
    second_gain = jnp.clip(1.0 + 0.18 * jax.random.normal(streams_of[17], (D,), jnp.float32), 0.1, 1.9)
    routes_keys = jax.random.split(jax.random.fold_in(streams_of[18], 1), TOKENS // TOKENS)
    routes_turns = jax.random.permutation(jax.random.fold_in(streams_of[18], 3), TOKENS // TOKENS)
    routes = jax.vmap(lambda own, number: deal_out(jax.random.fold_in(streams_of[18], 2), own, number, TOKENS, EXPERTS, TOPK, CAPACITY, 2))(routes_keys, routes_turns).reshape((TOKENS, TOPK))
    route_logits = draw_route_logits(jax.random.fold_in(streams_of[26], 71), 0)
    expert_gate = centred(streams_of[20], (EXPERTS, D, DE), (D // 16) ** -0.5, 0.5, ((0, 16), (2, 2)))
    expert_up = centred(streams_of[21], (EXPERTS, D, DE), (D // 16) ** -0.5, 0.5, ((0, 16), (2, 2)))
    expert_down = centred(streams_of[22], (EXPERTS, DE, D), (DE * 64) ** -0.5, 0.0234375, ((0, 16), (1, 2)))
    dense_up = centred(streams_of[23], (D, FD), D ** -0.5, 0.125, ((1, 32),))
    dense_down = centred(streams_of[24], (FD, D), FD ** -0.5, 0.09375, ((0, 32),))
    dense_gate = centred(streams_of[25], (D,), D ** -0.5, 0.125, (), jnp.float32)
    return dict(tokens=tokens, head_state=head_state, conv_state=conv_state, conv_proj_state=conv_proj_state, first_gain=first_gain, gate_weight=gate_weight, inner_weight=inner_weight, write_weight=write_weight, read_weight=read_weight, step_weight=step_weight, conv_kernel=conv_kernel, conv_proj_kernel=conv_proj_kernel, step_bias=step_bias, log_rate=log_rate, skip_gain=skip_gain, group_gain=group_gain, out_weight=out_weight, second_gain=second_gain, routes=routes, route_logits=route_logits, expert_gate=expert_gate, expert_up=expert_up, expert_down=expert_down, dense_up=dense_up, dense_down=dense_down, dense_gate=dense_gate)


norm_eps = 1e-05
clamp_limit = 7.0
glu_alpha = 1.702
highest = lax.Precision.HIGHEST

def rms_scale(values, gain_vec):
    return values * lax.rsqrt(lax.optimization_barrier(jnp.mean(values * values, axis=-1, keepdims=True)) + norm_eps) * gain_vec

def clamped_unit(gate_pre, up_pre):
    glu_part = jnp.minimum(gate_pre, clamp_limit)
    lin_part = jnp.clip(up_pre, -clamp_limit, clamp_limit)
    return glu_part * jax.nn.sigmoid(glu_alpha * glu_part) * (lin_part + 1.0)

def state_step(inner_proj, gate_proj, write_proj, read_proj, step_raw, conv_state, conv_proj_state, conv_kernel, conv_proj_kernel, step_bias, log_rate, skip_gain, group_gain, head_state, group_count):
    window_inner = jnp.concatenate([conv_state, inner_proj[:, None, :]], axis=1)
    window_proj = jnp.concatenate([conv_proj_state, jnp.stack([write_proj, read_proj], axis=1)[:, None]], axis=1)
    conv_inner = jax.nn.silu(lax.optimization_barrier(jnp.sum(window_inner.astype(jnp.float32) * conv_kernel[None], axis=1)))
    conv_proj = jax.nn.silu(lax.optimization_barrier(jnp.sum(window_proj.astype(jnp.float32) * conv_proj_kernel[None], axis=1)))
    seq_count, channels = conv_inner.shape
    head_count = step_raw.shape[1]
    head_width = channels // head_count
    state_width = conv_proj.shape[2] // group_count
    per_group = head_count // group_count
    head_input = conv_inner.reshape(seq_count, head_count, head_width)
    write_heads = jnp.repeat(conv_proj[:, 0].reshape(seq_count, group_count, state_width), per_group, axis=1)
    read_heads = jnp.repeat(conv_proj[:, 1].reshape(seq_count, group_count, state_width), per_group, axis=1)
    step_size = jax.nn.softplus(step_raw + step_bias)
    decay_rate = jnp.exp(-jnp.exp(log_rate) * step_size)
    state_out = decay_rate[:, :, None, None] * head_state + (step_size[:, :, None] * head_input)[:, :, :, None] * write_heads[:, :, None, :]
    read_out = jnp.einsum('shpn,shn->shp', state_out, read_heads, precision=highest) + skip_gain[None, :, None] * head_input
    gated_rows = read_out.reshape(seq_count, channels) * jax.nn.silu(gate_proj.astype(jnp.float32))
    grouped = gated_rows.reshape(seq_count, group_count, channels // group_count)
    grouped = grouped * lax.rsqrt(lax.optimization_barrier(jnp.mean(grouped * grouped, axis=-1, keepdims=True)) + norm_eps)
    mixer_rows = (grouped.reshape(seq_count, channels) * group_gain).astype(jnp.bfloat16)
    return (mixer_rows, state_out, window_inner[:, 1:], window_proj[:, 1:])

def reference(tokens, head_state, conv_state, conv_proj_state, first_gain, gate_weight, inner_weight, write_weight, read_weight, step_weight, conv_kernel, conv_proj_kernel, step_bias, log_rate, skip_gain, group_gain, out_weight, second_gain, routes, route_logits, expert_gate, expert_up, expert_down, dense_up, dense_down, dense_gate):
    normed_in = rms_scale(tokens.astype(jnp.float32), first_gain).astype(jnp.bfloat16)
    gate_proj = jnp.dot(normed_in, gate_weight, preferred_element_type=jnp.float32).astype(jnp.bfloat16)
    inner_proj = jnp.dot(normed_in, inner_weight, preferred_element_type=jnp.float32).astype(jnp.bfloat16)
    write_proj = jnp.dot(normed_in, write_weight, preferred_element_type=jnp.float32).astype(jnp.bfloat16)
    read_proj = jnp.dot(normed_in, read_weight, preferred_element_type=jnp.float32).astype(jnp.bfloat16)
    step_raw = jnp.dot(normed_in, step_weight, preferred_element_type=jnp.float32)
    mixer_rows, state_out, conv_out, conv_proj_out = state_step(inner_proj, gate_proj, write_proj, read_proj, step_raw, conv_state, conv_proj_state, conv_kernel, conv_proj_kernel, step_bias, log_rate, skip_gain, group_gain, head_state, GROUPS)
    mixed = jnp.dot(mixer_rows, out_weight, preferred_element_type=jnp.float32)
    hidden = (tokens.astype(jnp.float32) + mixed).astype(jnp.bfloat16)
    normed_mid = rms_scale(hidden.astype(jnp.float32), second_gain).astype(jnp.bfloat16)
    route_gates = jax.nn.softmax(route_logits.astype(jnp.float32), axis=-1)
    row_ids = jnp.arange(TOKENS, dtype=jnp.int32)

    def expert_pass(running, inputs):
        gate_block, up_block, down_block, expert_id = inputs
        route_hits = routes == expert_id
        row_weight = lax.optimization_barrier(jnp.sum(jnp.where(route_hits, route_gates, 0.0), axis=1))
        chosen = jnp.any(route_hits, axis=1)
        picked = jnp.argsort(jnp.where(chosen, row_ids, row_ids + TOKENS)).astype(jnp.int32)[:CAPACITY]
        picked_rows = normed_mid[picked]
        activated = clamped_unit(jnp.dot(picked_rows, gate_block, preferred_element_type=jnp.float32), jnp.dot(picked_rows, up_block, preferred_element_type=jnp.float32)).astype(jnp.bfloat16)
        expert_rows = jnp.dot(activated, down_block, preferred_element_type=jnp.float32) * row_weight[picked][:, None]
        return (running.at[picked].add(expert_rows), None)
    expert_ids = jnp.arange(EXPERTS, dtype=jnp.int32)
    expert_mix = lax.scan(expert_pass, jnp.zeros((TOKENS, D), jnp.float32), (expert_gate, expert_up, expert_down, expert_ids))[0]
    dense_act = jax.nn.silu(jnp.dot(normed_mid, dense_up, preferred_element_type=jnp.float32)).astype(jnp.bfloat16)
    dense_weight = jax.nn.sigmoid(jnp.dot(normed_mid.astype(jnp.float32), dense_gate, precision=highest))
    dense_value = jnp.dot(dense_act, dense_down, preferred_element_type=jnp.float32)
    layer_out = (hidden.astype(jnp.float32) + expert_mix + dense_weight[:, None] * dense_value).astype(jnp.bfloat16)
    return (layer_out, state_out, conv_out, conv_proj_out)
```

```python
import jax
import jax.numpy as jnp
from jax import lax
from jax.sharding import PartitionSpec as P

GROUPS = 4
TAIL = 128

norm_eps = 1e-05
clamp_limit = 7.0
glu_alpha = 1.702
highest = lax.Precision.HIGHEST
f32 = jnp.float32
bf16 = jnp.bfloat16


def clamped_unit(gate_pre, up_pre):
    glu_part = jnp.minimum(gate_pre, clamp_limit)
    lin_part = jnp.clip(up_pre, -clamp_limit, clamp_limit)
    return glu_part * jax.nn.sigmoid(glu_alpha * glu_part) * (lin_part + 1.0)


def state_step(
    inner_proj,
    gate_proj,
    write_proj,
    read_proj,
    step_raw,
    conv_state,
    conv_proj_state,
    conv_kernel,
    conv_proj_kernel,
    step_bias,
    log_rate,
    skip_gain,
    group_gain,
    head_state,
    group_count,
):
    window_inner = jnp.concatenate([conv_state, inner_proj[:, None, :]], axis=1)
    window_proj = jnp.concatenate(
        [conv_proj_state, jnp.stack([write_proj, read_proj], axis=1)[:, None]], axis=1
    )
    conv_inner = jax.nn.silu(jnp.sum(window_inner.astype(f32) * conv_kernel[None], axis=1))
    conv_proj = jax.nn.silu(jnp.sum(window_proj.astype(f32) * conv_proj_kernel[None], axis=1))
    seq_count, channels = conv_inner.shape
    head_count = step_raw.shape[1]
    head_width = channels // head_count
    state_width = conv_proj.shape[2] // group_count
    per_group = head_count // group_count
    head_input = conv_inner.reshape(seq_count, head_count, head_width)
    write_heads = jnp.repeat(
        conv_proj[:, 0].reshape(seq_count, group_count, state_width), per_group, axis=1
    )
    read_heads = jnp.repeat(
        conv_proj[:, 1].reshape(seq_count, group_count, state_width), per_group, axis=1
    )
    step_size = jax.nn.softplus(step_raw + step_bias)
    decay_rate = jnp.exp(-jnp.exp(log_rate) * step_size)
    state_out = (
        decay_rate[:, :, None, None] * head_state
        + (step_size[:, :, None] * head_input)[:, :, :, None] * write_heads[:, :, None, :]
    )
    read_out = (
        jnp.sum(state_out * read_heads[:, :, None, :], axis=-1)
        + skip_gain[None, :, None] * head_input
    )
    gated_rows = read_out.reshape(seq_count, channels) * jax.nn.silu(gate_proj.astype(f32))
    grouped = gated_rows.reshape(seq_count, group_count, channels // group_count)
    grouped = grouped * lax.rsqrt(jnp.mean(grouped * grouped, axis=-1, keepdims=True) + norm_eps)
    mixer_rows = (grouped.reshape(seq_count, channels) * group_gain).astype(bf16)
    return (mixer_rows, state_out, window_inner[:, 1:], window_proj[:, 1:])


def local(
    tokens,
    head_state,
    conv_state,
    conv_proj_state,
    first_gain,
    gate_weight,
    inner_weight,
    write_weight,
    read_weight,
    step_weight,
    conv_kernel,
    conv_proj_kernel,
    step_bias,
    log_rate,
    skip_gain,
    group_gain,
    out_weight,
    second_gain,
    routes,
    route_logits,
    expert_gate,
    expert_up,
    expert_down,
    dense_up,
    dense_down,
    dense_gate,
):
    n_ep = lax.axis_size("ep")
    n_tp = lax.axis_size("tp")
    n_all = n_ep * n_tp
    my_ep = lax.axis_index("ep")
    my_tp = lax.axis_index("tp")
    seq, width = tokens.shape
    rows = seq * n_ep
    half = gate_weight.shape[1]
    block = gate_weight.shape[0]

    raw_block = lax.all_to_all(tokens, "ep", split_axis=1, concat_axis=0, tiled=True)

    tok = tokens.astype(f32)
    scale = lax.rsqrt(jnp.mean(tok * tok, axis=-1, keepdims=True) + norm_eps)
    normed_in = (tok * scale * first_gain).astype(bf16)
    write_proj = jnp.dot(normed_in, write_weight, preferred_element_type=f32).astype(bf16)
    read_proj = jnp.dot(normed_in, read_weight, preferred_element_type=f32).astype(bf16)
    step_raw = jnp.dot(normed_in, step_weight, preferred_element_type=f32)

    swap = [(i, (i + 1) % n_tp) for i in range(n_tp)]
    other_weight = lax.ppermute(out_weight, "tp", swap)

    gain_block = lax.dynamic_slice_in_dim(first_gain, my_ep * block, block, 0)
    scaled = (raw_block.astype(f32) * gain_block).astype(bf16)
    terms = jnp.concatenate(
        [
            jnp.dot(scaled, gate_weight, preferred_element_type=f32).astype(bf16),
            jnp.dot(scaled, inner_weight, preferred_element_type=f32).astype(bf16),
        ],
        axis=1,
    ).reshape(n_ep, seq, 2 * half)
    terms = lax.all_to_all(terms, "ep", split_axis=0, concat_axis=0, tiled=True)
    both = jnp.sum(terms.astype(f32), axis=0) * scale
    gate_proj = both[:, :half].astype(bf16)
    inner_proj = both[:, half:].astype(bf16)

    mixer_rows, state_out, conv_out, conv_proj_out = state_step(
        inner_proj,
        gate_proj,
        write_proj,
        read_proj,
        step_raw,
        conv_state,
        conv_proj_state,
        conv_kernel,
        conv_proj_kernel,
        step_bias,
        log_rate,
        skip_gain,
        group_gain,
        head_state,
        GROUPS // n_tp,
    )

    top = routes.shape[1]
    tail = jnp.concatenate(
        [routes.astype(bf16), route_logits, jnp.zeros((seq, TAIL - 2 * top), bf16)], axis=1
    )
    packed = jnp.concatenate([mixer_rows, tail], axis=1)
    packed = jnp.broadcast_to(packed[None], (n_all, seq, half + TAIL))
    packed = lax.all_to_all(packed, ("ep", "tp"), split_axis=0, concat_axis=0, tiled=True)
    packed = packed.reshape(n_ep, n_tp, seq, half + TAIL)
    own_half = lax.dynamic_index_in_dim(packed, my_tp, 1, keepdims=False)
    other_half = lax.dynamic_index_in_dim(packed, n_tp - 1 - my_tp, 1, keepdims=False)
    own_half = own_half.reshape(rows, half + TAIL)
    other_half = other_half.reshape(rows, half + TAIL)
    all_routes = own_half[:, half : half + top]
    all_logits = own_half[:, half + top : half + 2 * top]
    mixed = jnp.dot(own_half[:, :half], out_weight, preferred_element_type=f32) + jnp.dot(
        other_half[:, :half], other_weight, preferred_element_type=f32
    )
    hidden_block = (raw_block.astype(f32) + mixed).astype(bf16)

    hidden = jnp.broadcast_to(hidden_block[None], (n_ep, rows, block))
    hidden = lax.all_to_all(hidden, "ep", split_axis=0, concat_axis=0, tiled=True)
    hidden = hidden.transpose(1, 0, 2).reshape(rows, width)

    hid = hidden.astype(f32)
    normed = hid * lax.rsqrt(jnp.mean(hid * hid, axis=-1, keepdims=True) + norm_eps) * second_gain
    normed_mid = normed.astype(bf16)

    route_gates = jax.nn.softmax(all_logits.astype(f32), axis=-1)
    row_weight = jnp.sum(
        jnp.where(all_routes.astype(jnp.int32) == my_ep, route_gates, 0.0), axis=1, keepdims=True
    )
    dense_weight = jax.nn.sigmoid(
        jnp.sum(normed_mid.astype(f32) * dense_gate, axis=-1, keepdims=True)
    )
    activated = clamped_unit(
        jnp.dot(normed_mid, expert_gate[0], preferred_element_type=f32),
        jnp.dot(normed_mid, expert_up[0], preferred_element_type=f32),
    ).astype(bf16)
    dense_inner = jax.nn.silu(
        jnp.dot(normed_mid, dense_up, preferred_element_type=f32)
    ).astype(bf16)
    total = (
        jnp.dot(activated, expert_down[0], preferred_element_type=f32) * row_weight
        + jnp.dot(dense_inner, dense_down, preferred_element_type=f32) * dense_weight
    ).astype(bf16)

    row_share = rows // n_all
    total = total.reshape(n_all, row_share, width)
    total = lax.all_to_all(total, ("ep", "tp"), split_axis=0, concat_axis=0, tiled=True)
    summed = jnp.sum(total.astype(f32), axis=0)
    own_rows = lax.dynamic_slice_in_dim(
        hidden, (my_ep * n_tp + my_tp) * row_share, row_share, 0
    )
    layer_out = (own_rows.astype(f32) + summed).astype(bf16)
    return (layer_out, state_out, conv_out, conv_proj_out)


def solution(mesh):
    placed = (
        P("ep", None),
        P("ep", "tp", None, None),
        P("ep", None, "tp"),
        P("ep", None, None, "tp"),
        P(),
        P("ep", "tp"),
        P("ep", "tp"),
        P(None, "tp"),
        P(None, "tp"),
        P(None, "tp"),
        P(None, "tp"),
        P(None, None, "tp"),
        P("tp"),
        P("tp"),
        P("tp"),
        P("tp"),
        P("tp", "ep"),
        P(),
        P("ep", None),
        P("ep", None),
        P("ep", None, "tp"),
        P("ep", None, "tp"),
        P("ep", "tp", None),
        P(None, ("ep", "tp")),
        P(("ep", "tp"), None),
        P(),
    )
    return jax.shard_map(
        local,
        mesh=mesh,
        in_specs=placed,
        out_specs=(
            P(("ep", "tp"), None),
            P("ep", "tp", None, None),
            P("ep", None, "tp"),
            P("ep", None, None, "tp"),
        ),
        check_vma=False,
    )
```

```python
import functools

import jax
import jax.numpy as jnp
from jax import lax
from jax.experimental import pallas as pl
from jax.experimental.pallas import tpu as pltpu
from jax.sharding import PartitionSpec as P

GROUPS = 4
TAIL = 128
LANES = 128
WORK = 5 * 10**9

norm_eps = 1e-05
clamp_limit = 7.0
glu_alpha = 1.702
highest = lax.Precision.HIGHEST
f32 = jnp.float32
bf16 = jnp.bfloat16


def clamped_unit(gate_pre, up_pre):
    glu_part = jnp.minimum(gate_pre, clamp_limit)
    lin_part = jnp.clip(up_pre, -clamp_limit, clamp_limit)
    return glu_part * jax.nn.sigmoid(glu_alpha * glu_part) * (lin_part + 1.0)


def state_step(
    inner_proj,
    gate_proj,
    write_proj,
    read_proj,
    step_raw,
    conv_state,
    conv_proj_state,
    conv_kernel,
    conv_proj_kernel,
    step_bias,
    log_rate,
    skip_gain,
    group_gain,
    head_state,
    group_count,
):
    window_inner = jnp.concatenate([conv_state, inner_proj[:, None, :]], axis=1)
    window_proj = jnp.concatenate(
        [conv_proj_state, jnp.stack([write_proj, read_proj], axis=1)[:, None]], axis=1
    )
    conv_inner = jax.nn.silu(jnp.sum(window_inner.astype(f32) * conv_kernel[None], axis=1))
    conv_proj = jax.nn.silu(jnp.sum(window_proj.astype(f32) * conv_proj_kernel[None], axis=1))
    seq_count, channels = conv_inner.shape
    head_count = step_raw.shape[1]
    head_width = channels // head_count
    state_width = conv_proj.shape[2] // group_count
    per_group = head_count // group_count
    head_input = conv_inner.reshape(seq_count, head_count, head_width)
    write_heads = jnp.repeat(
        conv_proj[:, 0].reshape(seq_count, group_count, state_width), per_group, axis=1
    )
    read_heads = jnp.repeat(
        conv_proj[:, 1].reshape(seq_count, group_count, state_width), per_group, axis=1
    )
    step_size = jax.nn.softplus(step_raw + step_bias)
    decay_rate = jnp.exp(-jnp.exp(log_rate) * step_size)
    state_out = (
        decay_rate[:, :, None, None] * head_state
        + (step_size[:, :, None] * head_input)[:, :, :, None] * write_heads[:, :, None, :]
    )
    read_out = (
        jnp.sum(state_out * read_heads[:, :, None, :], axis=-1)
        + skip_gain[None, :, None] * head_input
    )
    gated_rows = read_out.reshape(seq_count, channels) * jax.nn.silu(gate_proj.astype(f32))
    grouped = gated_rows.reshape(seq_count, group_count, channels // group_count)
    grouped = grouped * lax.rsqrt(jnp.mean(grouped * grouped, axis=-1, keepdims=True) + norm_eps)
    mixer_rows = (grouped.reshape(seq_count, channels) * group_gain).astype(bf16)
    return (mixer_rows, state_out, window_inner[:, 1:], window_proj[:, 1:])


def early_kernel(
    tokens_ref,
    gain_ref,
    write_ref,
    read_ref,
    step_ref,
    conv_state_ref,
    proj_state_ref,
    kernel_ref,
    proj_kernel_ref,
    bias_ref,
    rate_ref,
    skip_ref,
    group_gain_ref,
    routes_ref,
    logits_ref,
    state_ref,
    rows_ref,
    vec_ref,
    tail_ref,
    proj_out_ref,
    buf_ref,
    wait_state,
):
    taps = kernel_ref.shape[0]
    seq, width = tokens_ref.shape
    heads = bias_ref.shape[1]
    channels = kernel_ref.shape[1]
    head_width, state_width = state_ref.shape[2:]
    groups = write_ref.shape[1] // state_width
    per_group = heads // groups
    span = per_group * head_width
    blocks = channels // LANES

    tok = tokens_ref[...].astype(f32)
    scale = lax.rsqrt(jnp.sum(tok * tok, axis=1, keepdims=True) / width + norm_eps)
    normed = (tok * scale * gain_ref[...]).astype(bf16)

    tail_ref[...] = jnp.zeros(tail_ref.shape, f32)
    top = routes_ref.shape[1]
    tail_ref[:, 0:top] = routes_ref[...].astype(f32)
    tail_ref[:, top : 2 * top] = logits_ref[...].astype(f32)

    write = jnp.dot(normed, write_ref[...], preferred_element_type=f32).astype(bf16)
    read = jnp.dot(normed, read_ref[...], preferred_element_type=f32).astype(bf16)
    step = lax.dot_general(
        normed, step_ref[...], (((1,), (1,)), ((), ())), preferred_element_type=f32
    )
    step = step + bias_ref[...]
    dt = jnp.maximum(step, 0.0) + jnp.log1p(jnp.exp(-jnp.abs(step)))
    decay = jnp.exp(-jnp.exp(rate_ref[...]) * dt)

    for t in range(taps - 2):
        proj_out_ref[:, t] = proj_state_ref[:, t + 1]
    for t in range(seq):
        proj_out_ref[t, taps - 2, 0:1, :] = write[t : t + 1]
        proj_out_ref[t, taps - 2, 1:2, :] = read[t : t + 1]
        for i, new in ((0, write), (1, read)):
            total = new[t : t + 1].astype(f32) * proj_kernel_ref[taps - 1, i : i + 1, :]
            for j in range(taps - 1):
                total += (
                    proj_state_ref[t, j, i : i + 1, :].astype(f32)
                    * proj_kernel_ref[j, i : i + 1, :]
                )
            vec_ref[i, t : t + 1, :] = total * jax.nn.sigmoid(total)

    head = lax.broadcasted_iota(jnp.int32, (heads, channels), 0)
    chan = lax.broadcasted_iota(jnp.int32, (heads, channels), 1)
    spread = jnp.where(chan // head_width == head, 1.0, 0.0)

    def wide(v):
        return jnp.dot(v, spread, precision=highest, preferred_element_type=f32)

    dt_wide = wide(dt)
    decay_wide = wide(decay)
    skip_wide = wide(jnp.broadcast_to(skip_ref[...], (seq, heads)))

    def place(index, v):
        for c in range(blocks):
            rows_ref[index, c * seq : (c + 1) * seq, :] = v[:, c * LANES : (c + 1) * LANES]

    conv = jnp.zeros((seq, channels), f32)
    for j in range(taps - 1):
        conv += conv_state_ref[j].astype(f32) * kernel_ref[j : j + 1, :]
    place(0, conv)
    place(1, jnp.broadcast_to(kernel_ref[taps - 1 : taps, :], (seq, channels)))

    wait_state()
    for t in range(seq):
        for g in range(groups):
            cols = slice(g * state_width, (g + 1) * state_width)
            lanes = slice(g * span, (g + 1) * span)
            read_vec = vec_ref[1, t : t + 1, cols]
            read_hi = read_vec.astype(bf16)
            read_lo = (read_vec - read_hi.astype(f32)).astype(bf16)
            old = state_ref[t, g * per_group : (g + 1) * per_group].reshape(span, state_width)
            old_hi = old.astype(bf16)
            old_lo = (old - old_hi.astype(f32)).astype(bf16)

            def along(x, y):
                return lax.dot_general(
                    x, y, (((1,), (1,)), ((), ())), preferred_element_type=f32
                )

            sums = along(read_hi, old_hi) + along(read_hi, old_lo) + along(read_lo, old_hi)
            buf_ref[t : t + 1, lanes] = sums
            meet = jnp.sum(vec_ref[0, t : t + 1, cols] * read_vec, axis=1, keepdims=True)
            buf_ref[seq + t : seq + t + 1, lanes] = jnp.broadcast_to(meet, (1, span))
    place(2, decay_wide * buf_ref[0:seq, :])
    place(3, dt_wide * buf_ref[seq : 2 * seq, :] + skip_wide)
    place(4, jnp.broadcast_to(group_gain_ref[...], (seq, channels)))
    place(5, jnp.broadcast_to(scale, (seq, channels)))
    place(6, dt_wide)
    place(7, decay_wide)


def early_stage(count, *refs):
    sources, outs = refs[:count], refs[count : count + 4]
    buf_ref, places, sems = refs[count + 4], refs[count + 5 : -1], refs[-1]
    copies = [
        pltpu.make_async_copy(source, place, sems.at[i])
        for i, (source, place) in enumerate(zip(sources, places))
    ]
    for copy in copies:
        copy.start()
    for copy in copies[:-1]:
        copy.wait()
    early_kernel(*places, *outs, buf_ref, copies[-1].wait)


def project_kernel(
    raw_ref, gain_ref, gate_ref, inner_ref, tail_ref, out_ref, tok_ref, in_ref, buf_ref
):
    count, rows, lanes = out_ref.shape
    seq = tail_ref.shape[0]
    blocks = gate_ref.shape[1] // lanes
    in_ref[...] = raw_ref[...].astype(f32)
    for t in range(seq):
        tok_ref[t * count : (t + 1) * count, :] = in_ref[pl.ds(t, count, stride=seq), :]
    x = (tok_ref[...] * gain_ref[...]).astype(bf16)
    for i, weight in ((0, gate_ref), (1, inner_ref)):
        y = jnp.dot(x, weight[...], preferred_element_type=f32)
        for c in range(blocks):
            for t in range(seq):
                buf_ref[pl.ds((i * blocks + c) * seq + t, count, stride=rows), :] = y[
                    t * count : (t + 1) * count, c * lanes : (c + 1) * lanes
                ]
    last = 2 * blocks * seq
    tail = jnp.concatenate([tail_ref[...], jnp.zeros((rows - last - seq, lanes), f32)], axis=0)
    for p in range(count):
        buf_ref[p * rows + last : (p + 1) * rows, :] = tail
        out_ref[p] = buf_ref[p * rows : (p + 1) * rows, :].astype(bf16)


def mixer_kernel(seq, terms_ref, pre_ref, out_ref, conv_ref, inner_ref, tail_ref, buf_ref):
    count, rows, lanes = terms_ref.shape
    n_all, half, _ = out_ref.shape
    total = jnp.zeros((2 * half, lanes), f32)
    for p in range(count):
        total += terms_ref[p, 0 : 2 * half, :].astype(f32)
        buf_ref[p * 8 : (p + 1) * 8, :] = terms_ref[p, 2 * half : 2 * half + 8, :].astype(f32)
    for t in range(seq):
        tail_ref[t * count : (t + 1) * count, :] = buf_ref[pl.ds(t, count, stride=8), :]
    scale = pre_ref[5]
    gate = (total[0:half] * scale).astype(bf16).astype(f32)
    inner = (total[half : 2 * half] * scale).astype(bf16).astype(f32)
    conv = pre_ref[0] + pre_ref[1] * inner
    conv = conv * jax.nn.sigmoid(conv)
    conv_ref[...] = conv
    inner_ref[...] = inner
    gated = (pre_ref[2] + pre_ref[3] * conv) * (gate * jax.nn.sigmoid(gate))
    groups = GROUPS // lax.axis_size("tp")
    span = half // groups
    for g in range(groups):
        part = gated[g * span : (g + 1) * span]
        square = jnp.sum(part * part, axis=1, keepdims=True)
        square = jnp.broadcast_to(square, (span, lanes))
        whole = square
        for k in range(1, span // seq):
            whole += pltpu.roll(square, k * seq, 0)
        part = part * lax.rsqrt(whole / (span // seq * lanes) + norm_eps)
        buf_ref[g * span : (g + 1) * span, :] = part * pre_ref[4, g * span : (g + 1) * span, :]
    mixed = buf_ref[0:half, :].astype(bf16)
    for d in range(n_all):
        out_ref[d] = mixed


def hidden_kernel(
    count, seq, mix_ref, own_ref, other_ref, tok_ref, out_ref, buf_ref, lhs_ref
):
    n_all, half, lanes = mix_ref.shape
    n_tp = n_all // count
    my_tp = lax.axis_index("tp")
    for d in range(n_all):
        buf_ref[d * half : (d + 1) * half, :] = mix_ref[d].astype(f32)
    blocks = half // seq
    total = tok_ref[...]
    for which, weight in ((0, own_ref), (1, other_ref)):
        core = lax.rem(my_tp + which, n_tp)
        for c in range(blocks):
            for t in range(seq):
                lhs_ref[t * count : (t + 1) * count, c * lanes : (c + 1) * lanes] = buf_ref[
                    pl.ds(core * half + c * seq + t, count, stride=n_tp * half), :
                ].astype(bf16)
        total += jnp.dot(lhs_ref[...], weight[...], preferred_element_type=f32)
    hidden = total.astype(bf16)
    for p in range(count):
        out_ref[p] = hidden


def expert_kernel(
    top,
    seq,
    hid_ref,
    tail_ref,
    gain_ref,
    dgate_ref,
    gate_ref,
    up_ref,
    down_ref,
    dup_ref,
    ddown_ref,
    out_ref,
    own_ref,
    x_ref,
    h_ref,
    t_ref,
):
    blocks, rows, lanes = hid_ref.shape
    count = rows // seq
    my_ep = lax.axis_index("ep")
    own = lax.axis_index("tp") * count + my_ep
    total = jnp.zeros((rows, lanes), f32)
    for k in range(blocks):
        h = hid_ref[k].astype(f32)
        h_ref[k * rows : (k + 1) * rows, :] = h
        total += h * h
    scale = lax.rsqrt(jnp.sum(total, axis=1, keepdims=True) / (blocks * lanes) + norm_eps)
    dense = jnp.zeros((rows, lanes), f32)
    for k in range(blocks):
        h = h_ref[k * rows : (k + 1) * rows, :]
        x = (h * scale * gain_ref[k : k + 1, :]).astype(bf16)
        x_ref[:, k * lanes : (k + 1) * lanes] = x
        dense += x.astype(f32) * dgate_ref[k : k + 1, :]
    own_ref[...] = h_ref[pl.ds(own, blocks, stride=rows), :]
    dense_weight = jax.nn.sigmoid(jnp.sum(dense, axis=1, keepdims=True))

    tail = tail_ref[...]
    lane = lax.broadcasted_iota(jnp.int32, tail.shape, 1)
    scored = (lane >= top) & (lane < 2 * top)
    peak = jnp.max(jnp.where(scored, tail, -3e38), axis=1, keepdims=True)
    raised = jnp.where(scored, jnp.exp(jnp.minimum(tail - peak, 0.0)), 0.0)
    hits = (lane < top) & (tail.astype(jnp.int32) == my_ep)
    picked = jnp.where(hits, pltpu.roll(raised, lanes - top, 1), 0.0)
    row_weight = jnp.sum(picked, axis=1, keepdims=True) / jnp.sum(raised, axis=1, keepdims=True)

    x = x_ref[...]
    gate = jnp.dot(x, gate_ref[...], preferred_element_type=f32)
    up = jnp.dot(x, up_ref[...], preferred_element_type=f32)
    act = (clamped_unit(gate, up) * row_weight).astype(bf16)
    inner = jnp.dot(x, dup_ref[...], preferred_element_type=f32)
    dact = (inner * jax.nn.sigmoid(inner) * dense_weight).astype(bf16)
    for k in range(blocks):
        cols = slice(k * lanes, (k + 1) * lanes)
        y = jnp.dot(act, down_ref[:, cols], preferred_element_type=f32) + jnp.dot(
            dact, ddown_ref[:, cols], preferred_element_type=f32
        )
        for t in range(seq):
            t_ref[pl.ds(t * blocks + k, count, stride=seq * blocks), :] = y[
                t * count : (t + 1) * count
            ]
    for r in range(rows):
        out_ref[r] = t_ref[r * blocks : (r + 1) * blocks, :].astype(bf16)


def call(kernel, name, outs, args, scratch, limit, anywhere=(), sems=0, work=None):
    vmem = pl.BlockSpec(memory_space=pltpu.VMEM)
    hbm = pl.BlockSpec(memory_space=pltpu.HBM)
    args = [
        pltpu.with_memory_space_constraint(v, pltpu.HBM) if i in anywhere else v
        for i, v in enumerate(args)
    ]
    return pl.pallas_call(
        kernel,
        name=name,
        out_shape=tuple(jax.ShapeDtypeStruct(shape, kind) for shape, kind in outs),
        in_specs=[hbm if i in anywhere else vmem for i in range(len(args))],
        out_specs=tuple(vmem for _ in outs),
        scratch_shapes=[pltpu.VMEM(shape, kind) for shape, kind in scratch]
        + ([pltpu.SemaphoreType.DMA((sems,))] if sems else []),
        cost_estimate=work and pl.CostEstimate(
            flops=work, bytes_accessed=2**20, transcendentals=0
        ),
        compiler_params=pltpu.CompilerParams(vmem_limit_bytes=limit * 2**20),
    )(*args)


def final_kernel(terms_ref, own_ref, out_ref):
    count, blocks, lanes = terms_ref.shape
    total = own_ref[...]
    for r in range(count):
        total += terms_ref[r].astype(f32)
    for k in range(blocks):
        out_ref[:, k * lanes : (k + 1) * lanes] = total[k : k + 1, :].astype(bf16)


def final_stage(terms, own):
    count, blocks, lanes = terms.shape
    vmem = pl.BlockSpec(memory_space=pltpu.VMEM)
    return pl.pallas_call(
        final_kernel,
        name="final_stage",
        out_shape=jax.ShapeDtypeStruct((1, blocks * lanes), bf16),
        in_specs=[vmem] * 2,
        out_specs=vmem,
        compiler_params=pltpu.CompilerParams(vmem_limit_bytes=4 * 2**20),
    )(terms, own)


def direct(
    tokens,
    head_state,
    conv_state,
    conv_proj_state,
    first_gain,
    gate_weight,
    inner_weight,
    write_weight,
    read_weight,
    step_weight,
    conv_kernel,
    conv_proj_kernel,
    step_bias,
    log_rate,
    skip_gain,
    group_gain,
    out_weight,
    second_gain,
    routes,
    route_logits,
    expert_gate,
    expert_up,
    expert_down,
    dense_up,
    dense_down,
    dense_gate,
):
    n_ep = lax.axis_size("ep")
    n_tp = lax.axis_size("tp")
    n_all = n_ep * n_tp
    my_ep = lax.axis_index("ep")
    seq, width = tokens.shape
    rows = seq * n_ep
    channels = gate_weight.shape[1]
    half = channels // LANES * seq
    taps = conv_kernel.shape[0]
    heads = step_weight.shape[1]
    state_cols = write_weight.shape[1]
    top = routes.shape[1]
    head_width, state_width = head_state.shape[2:]
    groups = state_cols // state_width

    raw = lax.all_to_all(tokens, "ep", split_axis=1, concat_axis=0, tiled=True)

    other_weight = lax.ppermute(out_weight, "tp", [(i, (i + 1) % n_tp) for i in range(n_tp)])
    gain_block = lax.dynamic_slice_in_dim(first_gain, my_ep * LANES, LANES, 0)
    operands = (
        tokens,
        first_gain.reshape(1, width),
        write_weight,
        read_weight,
        step_weight.T,
        conv_state.transpose(1, 0, 2),
        conv_proj_state,
        conv_kernel,
        conv_proj_kernel,
        step_bias.reshape(1, heads),
        log_rate.reshape(1, heads),
        skip_gain.reshape(1, heads),
        group_gain.reshape(1, channels),
        routes,
        route_logits,
        head_state,
    )
    early, vectors, tail, proj_out = call(
        functools.partial(early_stage, len(operands)),
        "early",
        (
            ((8, half, LANES), f32),
            ((2, seq, state_cols), f32),
            ((seq, LANES), f32),
            (conv_proj_state.shape, bf16),
        ),
        operands,
        (((2 * seq, channels), f32), *((v.shape, v.dtype) for v in operands)),
        10,
        range(len(operands)),
        len(operands),
    )

    raw, other_weight = lax.optimization_barrier((raw, other_weight))
    terms, tok_block = call(
        project_kernel,
        "project",
        (((n_ep, 2 * half + 8, LANES), bf16), ((rows, LANES), f32)),
        (raw, gain_block.reshape(1, LANES), gate_weight, inner_weight, tail),
        (((rows, LANES), f32), ((n_ep * (2 * half + 8), LANES), f32)),
        6,
        work=WORK,
    )
    terms = lax.all_to_all(terms, "ep", split_axis=0, concat_axis=0, tiled=True)

    mixed, conv, inner, tails = call(
        functools.partial(mixer_kernel, seq),
        "mixer",
        (
            ((n_all, half, LANES), bf16),
            ((half, LANES), f32),
            ((half, LANES), f32),
            ((rows, LANES), f32),
        ),
        (terms, early),
        (((max(n_ep * 8, half), LANES), f32),),
        4,
        work=WORK,
    )
    mixed = lax.all_to_all(mixed, ("ep", "tp"), split_axis=0, concat_axis=0, tiled=True)

    (hidden,) = call(
        functools.partial(hidden_kernel, n_ep, seq),
        "hidden",
        (((n_ep, rows, LANES), bf16),),
        (mixed, out_weight, other_weight, tok_block),
        (((n_all * half, LANES), f32), ((rows, channels), bf16)),
        6,
        work=WORK,
    )
    hidden = lax.all_to_all(hidden, "ep", split_axis=0, concat_axis=0, tiled=True)

    terms, own_row = call(
        functools.partial(expert_kernel, top, seq),
        "experts",
        (((rows, n_ep, LANES), bf16), ((n_ep, LANES), f32)),
        (
            hidden,
            tails,
            second_gain.reshape(n_ep, LANES),
            dense_gate.reshape(n_ep, LANES),
            expert_gate[0],
            expert_up[0],
            expert_down[0],
            dense_up,
            dense_down,
        ),
        (
            ((rows, width), bf16),
            ((rows * n_ep, LANES), f32),
            ((rows * n_ep, LANES), f32),
        ),
        6,
    )
    terms = lax.all_to_all(terms, ("ep", "tp"), split_axis=0, concat_axis=0, tiled=True)

    conv, inner, early, vectors, own_row, conv_state, head_state = lax.optimization_barrier(
        (conv, inner, early, vectors, own_row, conv_state, head_state)
    )

    def by_head(v):
        v = v.reshape(channels // LANES, seq, LANES // head_width, head_width)
        return v.transpose(1, 0, 2, 3).reshape(seq, heads, head_width)

    write_heads = jnp.repeat(
        vectors[0].reshape(seq, groups, state_width), heads // groups, axis=1
    )
    state_out = (
        by_head(early[7])[:, :, :, None] * head_state
        + by_head(early[6] * conv)[:, :, :, None] * write_heads[:, :, None, :]
    )
    inner_rows = inner.reshape(channels // LANES, seq, LANES).transpose(1, 0, 2)
    inner_rows = inner_rows.reshape(seq, 1, channels).astype(bf16)
    conv_out = jnp.concatenate([conv_state[:, 1:], inner_rows], axis=1)

    layer_out = final_stage(terms, own_row)
    return (layer_out, state_out, conv_out, proj_out)


def local(
    tokens,
    head_state,
    conv_state,
    conv_proj_state,
    first_gain,
    gate_weight,
    inner_weight,
    write_weight,
    read_weight,
    step_weight,
    conv_kernel,
    conv_proj_kernel,
    step_bias,
    log_rate,
    skip_gain,
    group_gain,
    out_weight,
    second_gain,
    routes,
    route_logits,
    expert_gate,
    expert_up,
    expert_down,
    dense_up,
    dense_down,
    dense_gate,
):
    n_ep = lax.axis_size("ep")
    n_tp = lax.axis_size("tp")
    n_all = n_ep * n_tp
    my_ep = lax.axis_index("ep")
    my_tp = lax.axis_index("tp")
    seq, width = tokens.shape
    rows = seq * n_ep
    half = gate_weight.shape[1]
    block = gate_weight.shape[0]

    if block == LANES and n_all == rows and half % LANES == 0:
        return direct(
            tokens,
            head_state,
            conv_state,
            conv_proj_state,
            first_gain,
            gate_weight,
            inner_weight,
            write_weight,
            read_weight,
            step_weight,
            conv_kernel,
            conv_proj_kernel,
            step_bias,
            log_rate,
            skip_gain,
            group_gain,
            out_weight,
            second_gain,
            routes,
            route_logits,
            expert_gate,
            expert_up,
            expert_down,
            dense_up,
            dense_down,
            dense_gate,
        )

    raw_block = lax.all_to_all(tokens, "ep", split_axis=1, concat_axis=0, tiled=True)

    tok = tokens.astype(f32)
    scale = lax.rsqrt(jnp.mean(tok * tok, axis=-1, keepdims=True) + norm_eps)
    normed_in = (tok * scale * first_gain).astype(bf16)
    write_proj = jnp.dot(normed_in, write_weight, preferred_element_type=f32).astype(bf16)
    read_proj = jnp.dot(normed_in, read_weight, preferred_element_type=f32).astype(bf16)
    step_raw = jnp.dot(normed_in, step_weight, preferred_element_type=f32)

    swap = [(i, (i + 1) % n_tp) for i in range(n_tp)]
    other_weight = lax.ppermute(out_weight, "tp", swap)

    gain_block = lax.dynamic_slice_in_dim(first_gain, my_ep * block, block, 0)
    scaled = (raw_block.astype(f32) * gain_block).astype(bf16)
    terms = jnp.concatenate(
        [
            jnp.dot(scaled, gate_weight, preferred_element_type=f32).astype(bf16),
            jnp.dot(scaled, inner_weight, preferred_element_type=f32).astype(bf16),
        ],
        axis=1,
    ).reshape(n_ep, seq, 2 * half)
    terms = lax.all_to_all(terms, "ep", split_axis=0, concat_axis=0, tiled=True)
    both = jnp.sum(terms.astype(f32), axis=0) * scale
    gate_proj = both[:, :half].astype(bf16)
    inner_proj = both[:, half:].astype(bf16)

    mixer_rows, state_out, conv_out, conv_proj_out = state_step(
        inner_proj,
        gate_proj,
        write_proj,
        read_proj,
        step_raw,
        conv_state,
        conv_proj_state,
        conv_kernel,
        conv_proj_kernel,
        step_bias,
        log_rate,
        skip_gain,
        group_gain,
        head_state,
        GROUPS // n_tp,
    )

    top = routes.shape[1]
    tail = jnp.concatenate(
        [routes.astype(bf16), route_logits, jnp.zeros((seq, TAIL - 2 * top), bf16)], axis=1
    )
    packed = jnp.concatenate([mixer_rows, tail], axis=1)
    packed = jnp.broadcast_to(packed[None], (n_all, seq, half + TAIL))
    packed = lax.all_to_all(packed, ("ep", "tp"), split_axis=0, concat_axis=0, tiled=True)
    packed = packed.reshape(n_ep, n_tp, seq, half + TAIL)
    own_half = lax.dynamic_index_in_dim(packed, my_tp, 1, keepdims=False)
    other_half = lax.dynamic_index_in_dim(packed, n_tp - 1 - my_tp, 1, keepdims=False)
    own_half = own_half.reshape(rows, half + TAIL)
    other_half = other_half.reshape(rows, half + TAIL)
    all_routes = own_half[:, half : half + top]
    all_logits = own_half[:, half + top : half + 2 * top]
    mixed = jnp.dot(own_half[:, :half], out_weight, preferred_element_type=f32) + jnp.dot(
        other_half[:, :half], other_weight, preferred_element_type=f32
    )
    hidden_block = (raw_block.astype(f32) + mixed).astype(bf16)

    hidden = jnp.broadcast_to(hidden_block[None], (n_ep, rows, block))
    hidden = lax.all_to_all(hidden, "ep", split_axis=0, concat_axis=0, tiled=True)
    hidden = hidden.transpose(1, 0, 2).reshape(rows, width)

    hid = hidden.astype(f32)
    normed = hid * lax.rsqrt(jnp.mean(hid * hid, axis=-1, keepdims=True) + norm_eps) * second_gain
    normed_mid = normed.astype(bf16)

    route_gates = jax.nn.softmax(all_logits.astype(f32), axis=-1)
    row_weight = jnp.sum(
        jnp.where(all_routes.astype(jnp.int32) == my_ep, route_gates, 0.0), axis=1, keepdims=True
    )
    dense_weight = jax.nn.sigmoid(
        jnp.sum(normed_mid.astype(f32) * dense_gate, axis=-1, keepdims=True)
    )
    activated = clamped_unit(
        jnp.dot(normed_mid, expert_gate[0], preferred_element_type=f32),
        jnp.dot(normed_mid, expert_up[0], preferred_element_type=f32),
    ).astype(bf16)
    dense_inner = jax.nn.silu(
        jnp.dot(normed_mid, dense_up, preferred_element_type=f32)
    ).astype(bf16)
    total = (
        jnp.dot(activated, expert_down[0], preferred_element_type=f32) * row_weight
        + jnp.dot(dense_inner, dense_down, preferred_element_type=f32) * dense_weight
    ).astype(bf16)

    row_share = rows // n_all
    total = total.reshape(n_all, row_share, width)
    total = lax.all_to_all(total, ("ep", "tp"), split_axis=0, concat_axis=0, tiled=True)
    summed = jnp.sum(total.astype(f32), axis=0)
    own_rows = lax.dynamic_slice_in_dim(
        hidden, (my_ep * n_tp + my_tp) * row_share, row_share, 0
    )
    layer_out = (own_rows.astype(f32) + summed).astype(bf16)
    return (layer_out, state_out, conv_out, conv_proj_out)


def solution(mesh):
    placed = (
        P("ep", None),
        P("ep", "tp", None, None),
        P("ep", None, "tp"),
        P("ep", None, None, "tp"),
        P(),
        P("ep", "tp"),
        P("ep", "tp"),
        P(None, "tp"),
        P(None, "tp"),
        P(None, "tp"),
        P(None, "tp"),
        P(None, None, "tp"),
        P("tp"),
        P("tp"),
        P("tp"),
        P("tp"),
        P("tp", "ep"),
        P(),
        P("ep", None),
        P("ep", None),
        P("ep", None, "tp"),
        P("ep", None, "tp"),
        P("ep", "tp", None),
        P(None, ("ep", "tp")),
        P(("ep", "tp"), None),
        P(),
    )
    return jax.shard_map(
        local,
        mesh=mesh,
        in_specs=placed,
        out_specs=(
            P(("ep", "tp"), None),
            P("ep", "tp", None, None),
            P("ep", None, "tp"),
            P("ep", None, None, "tp"),
        ),
        check_vma=False,
    )
```

```python
import functools

import jax
import jax.numpy as jnp
from jax import lax
from jax.experimental import pallas as pl
from jax.experimental.pallas import tpu as pltpu
from jax.sharding import PartitionSpec as P

GROUPS = 4
TAIL = 128
LANES = 128
WORK = 5 * 10**9

norm_eps = 1e-05
clamp_limit = 7.0
glu_alpha = 1.702
highest = lax.Precision.HIGHEST
f32 = jnp.float32
bf16 = jnp.bfloat16


def clamped_unit(gate_pre, up_pre):
    glu_part = jnp.minimum(gate_pre, clamp_limit)
    lin_part = jnp.clip(up_pre, -clamp_limit, clamp_limit)
    return glu_part * jax.nn.sigmoid(glu_alpha * glu_part) * (lin_part + 1.0)


def state_step(
    inner_proj,
    gate_proj,
    write_proj,
    read_proj,
    step_raw,
    conv_state,
    conv_proj_state,
    conv_kernel,
    conv_proj_kernel,
    step_bias,
    log_rate,
    skip_gain,
    group_gain,
    head_state,
    group_count,
):
    window_inner = jnp.concatenate([conv_state, inner_proj[:, None, :]], axis=1)
    window_proj = jnp.concatenate(
        [conv_proj_state, jnp.stack([write_proj, read_proj], axis=1)[:, None]], axis=1
    )
    conv_inner = jax.nn.silu(jnp.sum(window_inner.astype(f32) * conv_kernel[None], axis=1))
    conv_proj = jax.nn.silu(jnp.sum(window_proj.astype(f32) * conv_proj_kernel[None], axis=1))
    seq_count, channels = conv_inner.shape
    head_count = step_raw.shape[1]
    head_width = channels // head_count
    state_width = conv_proj.shape[2] // group_count
    per_group = head_count // group_count
    head_input = conv_inner.reshape(seq_count, head_count, head_width)
    write_heads = jnp.repeat(
        conv_proj[:, 0].reshape(seq_count, group_count, state_width), per_group, axis=1
    )
    read_heads = jnp.repeat(
        conv_proj[:, 1].reshape(seq_count, group_count, state_width), per_group, axis=1
    )
    step_size = jax.nn.softplus(step_raw + step_bias)
    decay_rate = jnp.exp(-jnp.exp(log_rate) * step_size)
    state_out = (
        decay_rate[:, :, None, None] * head_state
        + (step_size[:, :, None] * head_input)[:, :, :, None] * write_heads[:, :, None, :]
    )
    read_out = (
        jnp.sum(state_out * read_heads[:, :, None, :], axis=-1)
        + skip_gain[None, :, None] * head_input
    )
    gated_rows = read_out.reshape(seq_count, channels) * jax.nn.silu(gate_proj.astype(f32))
    grouped = gated_rows.reshape(seq_count, group_count, channels // group_count)
    grouped = grouped * lax.rsqrt(jnp.mean(grouped * grouped, axis=-1, keepdims=True) + norm_eps)
    mixer_rows = (grouped.reshape(seq_count, channels) * group_gain).astype(bf16)
    return (mixer_rows, state_out, window_inner[:, 1:], window_proj[:, 1:])


def open_kernel(out_ref):
    out_ref[...] = jnp.zeros_like(out_ref)


def early_kernel(
    tokens_ref,
    gain_ref,
    write_ref,
    read_ref,
    step_ref,
    conv_state_ref,
    proj_state_ref,
    kernel_ref,
    proj_kernel_ref,
    bias_ref,
    rate_ref,
    skip_ref,
    group_gain_ref,
    routes_ref,
    logits_ref,
    state_ref,
    rows_ref,
    vec_ref,
    tail_ref,
    proj_out_ref,
    buf_ref,
    wait_state,
):
    taps = kernel_ref.shape[0]
    seq, width = tokens_ref.shape
    heads = bias_ref.shape[1]
    channels = kernel_ref.shape[1]
    head_width, state_width = state_ref.shape[2:]
    groups = write_ref.shape[1] // state_width
    per_group = heads // groups
    span = per_group * head_width
    blocks = channels // LANES

    tok = tokens_ref[...].astype(f32)
    scale = lax.rsqrt(jnp.sum(tok * tok, axis=1, keepdims=True) / width + norm_eps)
    normed = (tok * scale * gain_ref[...]).astype(bf16)
    write = jnp.dot(normed, write_ref[...], preferred_element_type=f32).astype(bf16)
    read = jnp.dot(normed, read_ref[...], preferred_element_type=f32).astype(bf16)
    step = lax.dot_general(
        normed, step_ref[...], (((1,), (1,)), ((), ())), preferred_element_type=f32
    )
    step = step + bias_ref[...]
    dt = jnp.maximum(step, 0.0) + jnp.log1p(jnp.exp(-jnp.abs(step)))
    decay = jnp.exp(-jnp.exp(rate_ref[...]) * dt)

    tail_ref[...] = jnp.zeros(tail_ref.shape, f32)
    top = routes_ref.shape[1]
    tail_ref[:, 0:top] = routes_ref[...].astype(f32)
    tail_ref[:, top : 2 * top] = logits_ref[...].astype(f32)

    for t in range(taps - 2):
        proj_out_ref[:, t] = proj_state_ref[:, t + 1]
    for t in range(seq):
        proj_out_ref[t, taps - 2, 0:1, :] = write[t : t + 1]
        proj_out_ref[t, taps - 2, 1:2, :] = read[t : t + 1]
        for i, new in ((0, write), (1, read)):
            total = new[t : t + 1].astype(f32) * proj_kernel_ref[taps - 1, i : i + 1, :]
            for j in range(taps - 1):
                total += (
                    proj_state_ref[t, j, i : i + 1, :].astype(f32)
                    * proj_kernel_ref[j, i : i + 1, :]
                )
            vec_ref[i, t : t + 1, :] = total * jax.nn.sigmoid(total)

    head = lax.broadcasted_iota(jnp.int32, (heads, channels), 0)
    chan = lax.broadcasted_iota(jnp.int32, (heads, channels), 1)
    spread = jnp.where(chan // head_width == head, 1.0, 0.0)

    def wide(v):
        return jnp.dot(v, spread, precision=highest, preferred_element_type=f32)

    dt_wide = wide(dt)
    decay_wide = wide(decay)
    skip_wide = wide(jnp.broadcast_to(skip_ref[...], (seq, heads)))

    def place(index, v):
        for c in range(blocks):
            rows_ref[index, c * seq : (c + 1) * seq, :] = v[:, c * LANES : (c + 1) * LANES]

    conv = jnp.zeros((seq, channels), f32)
    for j in range(taps - 1):
        conv += conv_state_ref[j].astype(f32) * kernel_ref[j : j + 1, :]
    place(0, conv)
    place(1, jnp.broadcast_to(kernel_ref[taps - 1 : taps, :], (seq, channels)))

    wait_state()
    for t in range(seq):
        for g in range(groups):
            cols = slice(g * state_width, (g + 1) * state_width)
            lanes = slice(g * span, (g + 1) * span)
            read_vec = vec_ref[1, t : t + 1, cols]
            read_hi = read_vec.astype(bf16)
            read_lo = (read_vec - read_hi.astype(f32)).astype(bf16)
            old = state_ref[t, g * per_group : (g + 1) * per_group].reshape(span, state_width)
            old_hi = old.astype(bf16)
            old_lo = (old - old_hi.astype(f32)).astype(bf16)

            def along(x, y):
                return lax.dot_general(
                    x, y, (((1,), (1,)), ((), ())), preferred_element_type=f32
                )

            sums = along(read_hi, old_hi) + along(read_hi, old_lo) + along(read_lo, old_hi)
            buf_ref[t : t + 1, lanes] = sums
            meet = jnp.sum(vec_ref[0, t : t + 1, cols] * read_vec, axis=1, keepdims=True)
            buf_ref[seq + t : seq + t + 1, lanes] = jnp.broadcast_to(meet, (1, span))
    place(2, decay_wide * buf_ref[0:seq, :])
    place(3, dt_wide * buf_ref[seq : 2 * seq, :] + skip_wide)
    place(4, jnp.broadcast_to(group_gain_ref[...], (seq, channels)))
    place(5, jnp.broadcast_to(scale, (seq, channels)))
    place(6, dt_wide)
    place(7, decay_wide)


def early_stage(count, *refs):
    sources, outs = refs[:count], refs[count + 1 : count + 5]
    buf_ref, state_ref, sems = refs[count + 5 :]
    copy = pltpu.make_async_copy(sources[-1], state_ref, sems.at[0])
    copy.start()
    early_kernel(*sources[:-1], state_ref, *outs, buf_ref, copy.wait)


def project_kernel(
    raw_ref, gain_ref, gate_ref, inner_ref, tail_ref, out_ref, tok_ref, in_ref, buf_ref
):
    count, rows, lanes = out_ref.shape
    seq = tail_ref.shape[0]
    blocks = gate_ref.shape[1] // lanes
    in_ref[...] = raw_ref[...].astype(f32)
    for t in range(seq):
        tok_ref[t * count : (t + 1) * count, :] = in_ref[pl.ds(t, count, stride=seq), :]
    gain = gain_ref[pl.ds(lax.axis_index("ep"), 1), :]
    x = (tok_ref[...] * gain).astype(bf16)
    for i, weight in ((0, gate_ref), (1, inner_ref)):
        y = jnp.dot(x, weight[...], preferred_element_type=f32)
        for c in range(blocks):
            for t in range(seq):
                buf_ref[pl.ds((i * blocks + c) * seq + t, count, stride=rows), :] = y[
                    t * count : (t + 1) * count, c * lanes : (c + 1) * lanes
                ]
    last = 2 * blocks * seq
    tail = jnp.concatenate([tail_ref[...], jnp.zeros((rows - last - seq, lanes), f32)], axis=0)
    for p in range(count):
        buf_ref[p * rows + last : (p + 1) * rows, :] = tail
        out_ref[p] = buf_ref[p * rows : (p + 1) * rows, :].astype(bf16)


def mixer_kernel(seq, terms_ref, pre_ref, out_ref, conv_ref, inner_ref, tail_ref, buf_ref):
    count, _, lanes = terms_ref.shape
    n_all, half, _ = out_ref.shape
    total = jnp.zeros((2 * half, lanes), f32)
    for p in range(count):
        total += terms_ref[p, 0 : 2 * half, :].astype(f32)
        buf_ref[p * 8 : (p + 1) * 8, :] = terms_ref[p, 2 * half : 2 * half + 8, :].astype(f32)
    for t in range(seq):
        tail_ref[t * count : (t + 1) * count, :] = buf_ref[pl.ds(t, count, stride=8), :]
    scale = pre_ref[5]
    gate = (total[0:half] * scale).astype(bf16).astype(f32)
    inner = (total[half : 2 * half] * scale).astype(bf16).astype(f32)
    conv = pre_ref[0] + pre_ref[1] * inner
    conv = conv * jax.nn.sigmoid(conv)
    conv_ref[...] = conv
    inner_ref[...] = inner
    gated = (pre_ref[2] + pre_ref[3] * conv) * (gate * jax.nn.sigmoid(gate))
    groups = GROUPS // lax.axis_size("tp")
    span = half // groups
    for g in range(groups):
        part = gated[g * span : (g + 1) * span]
        square = jnp.sum(part * part, axis=1, keepdims=True)
        square = jnp.broadcast_to(square, (span, lanes))
        whole = square
        for k in range(1, span // seq):
            whole += pltpu.roll(square, k * seq, 0)
        part = part * lax.rsqrt(whole / (span // seq * lanes) + norm_eps)
        buf_ref[g * span : (g + 1) * span, :] = part * pre_ref[4, g * span : (g + 1) * span, :]
    mixed = buf_ref[0:half, :].astype(bf16)
    for d in range(n_all):
        out_ref[d] = mixed


def hidden_kernel(
    count, mix_ref, own_ref, other_ref, tok_ref, out_ref, buf_ref, lhs_ref
):
    n_all, half, lanes = mix_ref.shape
    n_tp = n_all // count
    my_tp = lax.axis_index("tp")
    for d in range(n_all):
        buf_ref[d * half : (d + 1) * half, :] = mix_ref[d].astype(f32)
    blocks = lhs_ref.shape[1] // lanes
    seq = half // blocks
    total = tok_ref[pl.ds(pl.multiple_of(my_tp * count, count), count), :]
    for which, weight in ((0, own_ref), (1, other_ref)):
        core = lax.rem(my_tp + which, n_tp)
        for c in range(blocks):
            lhs_ref[:, c * lanes : (c + 1) * lanes] = buf_ref[
                pl.ds(core * half + c * seq + my_tp, count, stride=n_tp * half), :
            ].astype(bf16)
        total += jnp.dot(lhs_ref[...], weight[...], preferred_element_type=f32)
    hidden = total.astype(bf16)
    for d in range(n_all):
        out_ref[d] = hidden


def expert_kernel(
    top,
    seq,
    hid_ref,
    tail_ref,
    gain_ref,
    dgate_ref,
    gate_ref,
    up_ref,
    down_ref,
    dup_ref,
    ddown_ref,
    out_ref,
    own_ref,
    x_ref,
    h_ref,
    t_ref,
):
    count, lanes = hid_ref.shape[1:]
    rows = count * seq
    blocks = hid_ref.shape[0] // seq
    my_ep = lax.axis_index("ep")
    own = lax.axis_index("tp") * count + my_ep
    total = jnp.zeros((rows, lanes), f32)
    for k in range(blocks):
        for t in range(seq):
            at = k * rows + t * count
            h_ref[at : at + count, :] = hid_ref[k * seq + t].astype(f32)
        h = h_ref[k * rows : (k + 1) * rows, :]
        total += h * h
    scale = lax.rsqrt(jnp.sum(total, axis=1, keepdims=True) / (blocks * lanes) + norm_eps)
    dense = jnp.zeros((rows, lanes), f32)
    for k in range(blocks):
        h = h_ref[k * rows : (k + 1) * rows, :]
        x = (h * scale * gain_ref[k : k + 1, :]).astype(bf16)
        x_ref[:, k * lanes : (k + 1) * lanes] = x
        dense += x.astype(f32) * dgate_ref[k : k + 1, :]
    own_ref[...] = h_ref[pl.ds(own, blocks, stride=rows), :]
    dense_weight = jax.nn.sigmoid(jnp.sum(dense, axis=1, keepdims=True))

    tail = tail_ref[...]
    lane = lax.broadcasted_iota(jnp.int32, tail.shape, 1)
    scored = (lane >= top) & (lane < 2 * top)
    peak = jnp.max(jnp.where(scored, tail, -3e38), axis=1, keepdims=True)
    raised = jnp.where(scored, jnp.exp(jnp.minimum(tail - peak, 0.0)), 0.0)
    hits = (lane < top) & (tail.astype(jnp.int32) == my_ep)
    picked = jnp.where(hits, pltpu.roll(raised, lanes - top, 1), 0.0)
    row_weight = jnp.sum(picked, axis=1, keepdims=True) / jnp.sum(raised, axis=1, keepdims=True)

    x = x_ref[...]
    gate = jnp.dot(x, gate_ref[...], preferred_element_type=f32)
    up = jnp.dot(x, up_ref[...], preferred_element_type=f32)
    act = (clamped_unit(gate, up) * row_weight).astype(bf16)
    inner = jnp.dot(x, dup_ref[...], preferred_element_type=f32)
    dact = (inner * jax.nn.sigmoid(inner) * dense_weight).astype(bf16)
    for k in range(blocks):
        cols = slice(k * lanes, (k + 1) * lanes)
        y = jnp.dot(act, down_ref[:, cols], preferred_element_type=f32) + jnp.dot(
            dact, ddown_ref[:, cols], preferred_element_type=f32
        )
        for t in range(seq):
            t_ref[pl.ds(t * blocks + k, count, stride=seq * blocks), :] = y[
                t * count : (t + 1) * count
            ]
    for r in range(rows):
        out_ref[r] = t_ref[r * blocks : (r + 1) * blocks, :].astype(bf16)


def call(kernel, outs, args, scratch, limit, anywhere=(), sems=0, work=None):
    vmem = pl.BlockSpec(memory_space=pltpu.VMEM)
    hbm = pl.BlockSpec(memory_space=pltpu.HBM)
    args = [
        pltpu.with_memory_space_constraint(v, pltpu.HBM) if i in anywhere else v
        for i, v in enumerate(args)
    ]
    return pl.pallas_call(
        kernel,
        out_shape=tuple(jax.ShapeDtypeStruct(shape, kind) for shape, kind in outs),
        in_specs=[hbm if i in anywhere else vmem for i in range(len(args))],
        out_specs=tuple(vmem for _ in outs),
        scratch_shapes=[pltpu.VMEM(shape, kind) for shape, kind in scratch]
        + ([pltpu.SemaphoreType.DMA((sems,))] if sems else []),
        cost_estimate=work and pl.CostEstimate(
            flops=work, bytes_accessed=2**20, transcendentals=0
        ),
        compiler_params=pltpu.CompilerParams(vmem_limit_bytes=limit * 2**20),
    )(*args)


def final_kernel(terms_ref, own_ref, out_ref):
    count, blocks, lanes = terms_ref.shape
    total = own_ref[...]
    for r in range(count):
        total += terms_ref[r].astype(f32)
    for k in range(blocks):
        out_ref[:, k * lanes : (k + 1) * lanes] = total[k : k + 1, :].astype(bf16)


def final_stage(terms, own):
    _, blocks, lanes = terms.shape
    vmem = pl.BlockSpec(memory_space=pltpu.VMEM)
    return pl.pallas_call(
        final_kernel,
        name="final_stage",
        out_shape=jax.ShapeDtypeStruct((1, blocks * lanes), bf16),
        in_specs=[vmem] * 2,
        out_specs=vmem,
        compiler_params=pltpu.CompilerParams(vmem_limit_bytes=4 * 2**20),
    )(terms, own)


def direct(
    tokens,
    head_state,
    conv_state,
    conv_proj_state,
    first_gain,
    gate_weight,
    inner_weight,
    write_weight,
    read_weight,
    step_weight,
    conv_kernel,
    conv_proj_kernel,
    step_bias,
    log_rate,
    skip_gain,
    group_gain,
    out_weight,
    second_gain,
    routes,
    route_logits,
    expert_gate,
    expert_up,
    expert_down,
    dense_up,
    dense_down,
    dense_gate,
):
    n_ep = lax.axis_size("ep")
    n_tp = lax.axis_size("tp")
    n_all = n_ep * n_tp
    seq, width = tokens.shape
    rows = seq * n_ep
    channels = gate_weight.shape[1]
    half = channels // LANES * seq
    heads = step_weight.shape[1]
    state_cols = write_weight.shape[1]
    top = routes.shape[1]
    head_width, state_width = head_state.shape[2:]
    groups = state_cols // state_width

    raw = lax.all_to_all(tokens, "ep", split_axis=1, concat_axis=0, tiled=True)

    swap = [(i, (i + 1) % n_tp) for i in range(n_tp)]
    other_weight = lax.ppermute(out_weight, "tp", swap)

    operands = (
        tokens,
        first_gain.reshape(1, width),
        write_weight,
        read_weight,
        step_weight.T,
        conv_state.transpose(1, 0, 2),
        conv_proj_state,
        conv_kernel,
        conv_proj_kernel,
        step_bias.reshape(1, heads),
        log_rate.reshape(1, heads),
        skip_gain.reshape(1, heads),
        group_gain.reshape(1, channels),
        routes,
        route_logits,
        head_state,
    )
    (opened,) = call(open_kernel, (((8, LANES), f32),), (), (), 1, work=WORK)
    early, vectors, tail, proj_out = call(
        functools.partial(early_stage, len(operands)),
        (
            ((8, half, LANES), f32),
            ((2, seq, state_cols), f32),
            ((seq, LANES), f32),
            (conv_proj_state.shape, bf16),
        ),
        (*operands, opened),
        (((2 * seq, channels), f32), (head_state.shape, f32)),
        6,
        (len(operands) - 1,),
        1,
    )

    raw, other_weight = lax.optimization_barrier((raw, other_weight))
    terms, tok_block = call(
        project_kernel,
        (((n_ep, 2 * half + 8, LANES), bf16), ((rows, LANES), f32)),
        (raw, first_gain.reshape(n_ep, LANES), gate_weight, inner_weight, tail),
        (((rows, LANES), f32), ((n_ep * (2 * half + 8), LANES), f32)),
        6,
        work=WORK,
    )
    terms = lax.all_to_all(terms, "ep", split_axis=0, concat_axis=0, tiled=True)

    mixed, conv, inner, tails = call(
        functools.partial(mixer_kernel, seq),
        (
            ((n_all, half, LANES), bf16),
            ((half, LANES), f32),
            ((half, LANES), f32),
            ((rows, LANES), f32),
        ),
        (terms, early),
        (((max(n_ep * 8, half), LANES), f32),),
        4,
        work=WORK,
    )
    mixed = lax.all_to_all(mixed, ("ep", "tp"), split_axis=0, concat_axis=0, tiled=True)

    (hidden,) = call(
        functools.partial(hidden_kernel, n_ep),
        (((n_all, n_ep, LANES), bf16),),
        (mixed, out_weight, other_weight, tok_block),
        (((n_all * half, LANES), f32), ((n_ep, channels), bf16)),
        6,
        work=WORK,
    )
    hidden = lax.all_to_all(hidden, ("ep", "tp"), split_axis=0, concat_axis=0, tiled=True)

    terms, own_row = call(
        functools.partial(expert_kernel, top, seq),
        (((rows, n_ep, LANES), bf16), ((n_ep, LANES), f32)),
        (
            hidden,
            tails,
            second_gain.reshape(n_ep, LANES),
            dense_gate.reshape(n_ep, LANES),
            expert_gate[0],
            expert_up[0],
            expert_down[0],
            dense_up,
            dense_down,
        ),
        (
            ((rows, width), bf16),
            ((rows * n_ep, LANES), f32),
            ((rows * n_ep, LANES), f32),
        ),
        6,
    )
    terms = lax.all_to_all(terms, ("ep", "tp"), split_axis=0, concat_axis=0, tiled=True)

    conv, inner, early, vectors, own_row, conv_state, head_state = lax.optimization_barrier(
        (conv, inner, early, vectors, own_row, conv_state, head_state)
    )

    def by_head(v):
        v = v.reshape(channels // LANES, seq, LANES // head_width, head_width)
        return v.transpose(1, 0, 2, 3).reshape(seq, heads, head_width)

    write_heads = jnp.repeat(
        vectors[0].reshape(seq, groups, state_width), heads // groups, axis=1
    )
    state_out = (
        by_head(early[7])[:, :, :, None] * head_state
        + by_head(early[6] * conv)[:, :, :, None] * write_heads[:, :, None, :]
    )
    inner_rows = inner.reshape(channels // LANES, seq, LANES).transpose(1, 0, 2)
    inner_rows = inner_rows.reshape(seq, 1, channels).astype(bf16)
    conv_out = jnp.concatenate([conv_state[:, 1:], inner_rows], axis=1)

    layer_out = final_stage(terms, own_row)
    return (layer_out, state_out, conv_out, proj_out)


def local(
    tokens,
    head_state,
    conv_state,
    conv_proj_state,
    first_gain,
    gate_weight,
    inner_weight,
    write_weight,
    read_weight,
    step_weight,
    conv_kernel,
    conv_proj_kernel,
    step_bias,
    log_rate,
    skip_gain,
    group_gain,
    out_weight,
    second_gain,
    routes,
    route_logits,
    expert_gate,
    expert_up,
    expert_down,
    dense_up,
    dense_down,
    dense_gate,
):
    n_ep = lax.axis_size("ep")
    n_tp = lax.axis_size("tp")
    n_all = n_ep * n_tp
    my_ep = lax.axis_index("ep")
    my_tp = lax.axis_index("tp")
    seq, width = tokens.shape
    rows = seq * n_ep
    half = gate_weight.shape[1]
    block = gate_weight.shape[0]

    if block == LANES and n_all == rows and seq == n_tp and half % LANES == 0:
        return direct(
            tokens,
            head_state,
            conv_state,
            conv_proj_state,
            first_gain,
            gate_weight,
            inner_weight,
            write_weight,
            read_weight,
            step_weight,
            conv_kernel,
            conv_proj_kernel,
            step_bias,
            log_rate,
            skip_gain,
            group_gain,
            out_weight,
            second_gain,
            routes,
            route_logits,
            expert_gate,
            expert_up,
            expert_down,
            dense_up,
            dense_down,
            dense_gate,
        )

    raw_block = lax.all_to_all(tokens, "ep", split_axis=1, concat_axis=0, tiled=True)

    tok = tokens.astype(f32)
    scale = lax.rsqrt(jnp.mean(tok * tok, axis=-1, keepdims=True) + norm_eps)
    normed_in = (tok * scale * first_gain).astype(bf16)
    write_proj = jnp.dot(normed_in, write_weight, preferred_element_type=f32).astype(bf16)
    read_proj = jnp.dot(normed_in, read_weight, preferred_element_type=f32).astype(bf16)
    step_raw = jnp.dot(normed_in, step_weight, preferred_element_type=f32)

    swap = [(i, (i + 1) % n_tp) for i in range(n_tp)]
    other_weight = lax.ppermute(out_weight, "tp", swap)

    gain_block = lax.dynamic_slice_in_dim(first_gain, my_ep * block, block, 0)
    scaled = (raw_block.astype(f32) * gain_block).astype(bf16)
    terms = jnp.concatenate(
        [
            jnp.dot(scaled, gate_weight, preferred_element_type=f32).astype(bf16),
            jnp.dot(scaled, inner_weight, preferred_element_type=f32).astype(bf16),
        ],
        axis=1,
    ).reshape(n_ep, seq, 2 * half)
    terms = lax.all_to_all(terms, "ep", split_axis=0, concat_axis=0, tiled=True)
    both = jnp.sum(terms.astype(f32), axis=0) * scale
    gate_proj = both[:, :half].astype(bf16)
    inner_proj = both[:, half:].astype(bf16)

    mixer_rows, state_out, conv_out, conv_proj_out = state_step(
        inner_proj,
        gate_proj,
        write_proj,
        read_proj,
        step_raw,
        conv_state,
        conv_proj_state,
        conv_kernel,
        conv_proj_kernel,
        step_bias,
        log_rate,
        skip_gain,
        group_gain,
        head_state,
        GROUPS // n_tp,
    )

    top = routes.shape[1]
    tail = jnp.concatenate(
        [routes.astype(bf16), route_logits, jnp.zeros((seq, TAIL - 2 * top), bf16)], axis=1
    )
    packed = jnp.concatenate([mixer_rows, tail], axis=1)
    packed = jnp.broadcast_to(packed[None], (n_all, seq, half + TAIL))
    packed = lax.all_to_all(packed, ("ep", "tp"), split_axis=0, concat_axis=0, tiled=True)
    packed = packed.reshape(n_ep, n_tp, seq, half + TAIL)
    own_half = lax.dynamic_index_in_dim(packed, my_tp, 1, keepdims=False)
    other_half = lax.dynamic_index_in_dim(packed, n_tp - 1 - my_tp, 1, keepdims=False)
    own_half = own_half.reshape(rows, half + TAIL)
    other_half = other_half.reshape(rows, half + TAIL)
    all_routes = own_half[:, half : half + top]
    all_logits = own_half[:, half + top : half + 2 * top]
    mixed = jnp.dot(own_half[:, :half], out_weight, preferred_element_type=f32) + jnp.dot(
        other_half[:, :half], other_weight, preferred_element_type=f32
    )
    hidden_block = (raw_block.astype(f32) + mixed).astype(bf16)

    hidden = jnp.broadcast_to(hidden_block[None], (n_ep, rows, block))
    hidden = lax.all_to_all(hidden, "ep", split_axis=0, concat_axis=0, tiled=True)
    hidden = hidden.transpose(1, 0, 2).reshape(rows, width)

    hid = hidden.astype(f32)
    normed = hid * lax.rsqrt(jnp.mean(hid * hid, axis=-1, keepdims=True) + norm_eps) * second_gain
    normed_mid = normed.astype(bf16)

    route_gates = jax.nn.softmax(all_logits.astype(f32), axis=-1)
    row_weight = jnp.sum(
        jnp.where(all_routes.astype(jnp.int32) == my_ep, route_gates, 0.0), axis=1, keepdims=True
    )
    dense_weight = jax.nn.sigmoid(
        jnp.sum(normed_mid.astype(f32) * dense_gate, axis=-1, keepdims=True)
    )
    activated = clamped_unit(
        jnp.dot(normed_mid, expert_gate[0], preferred_element_type=f32),
        jnp.dot(normed_mid, expert_up[0], preferred_element_type=f32),
    ).astype(bf16)
    dense_inner = jax.nn.silu(
        jnp.dot(normed_mid, dense_up, preferred_element_type=f32)
    ).astype(bf16)
    total = (
        jnp.dot(activated, expert_down[0], preferred_element_type=f32) * row_weight
        + jnp.dot(dense_inner, dense_down, preferred_element_type=f32) * dense_weight
    ).astype(bf16)

    row_share = rows // n_all
    total = total.reshape(n_all, row_share, width)
    total = lax.all_to_all(total, ("ep", "tp"), split_axis=0, concat_axis=0, tiled=True)
    summed = jnp.sum(total.astype(f32), axis=0)
    own_rows = lax.dynamic_slice_in_dim(
        hidden, (my_ep * n_tp + my_tp) * row_share, row_share, 0
    )
    layer_out = (own_rows.astype(f32) + summed).astype(bf16)
    return (layer_out, state_out, conv_out, conv_proj_out)


def solution(mesh):
    placed = (
        P("ep", None),
        P("ep", "tp", None, None),
        P("ep", None, "tp"),
        P("ep", None, None, "tp"),
        P(),
        P("ep", "tp"),
        P("ep", "tp"),
        P(None, "tp"),
        P(None, "tp"),
        P(None, "tp"),
        P(None, "tp"),
        P(None, None, "tp"),
        P("tp"),
        P("tp"),
        P("tp"),
        P("tp"),
        P("tp", "ep"),
        P(),
        P("ep", None),
        P("ep", None),
        P("ep", None, "tp"),
        P("ep", None, "tp"),
        P("ep", "tp", None),
        P(None, ("ep", "tp")),
        P(("ep", "tp"), None),
        P(),
    )
    return jax.shard_map(
        local,
        mesh=mesh,
        in_specs=placed,
        out_specs=(
            P(("ep", "tp"), None),
            P("ep", "tp", None, None),
            P("ep", None, "tp"),
            P("ep", None, None, "tp"),
        ),
        check_vma=False,
    )
```

```python
import functools

import jax
import jax.numpy as jnp
from jax import lax
from jax.experimental import pallas as pl
from jax.experimental.pallas import tpu as pltpu
from jax.sharding import PartitionSpec as P

GROUPS = 4
TAIL = 128
LANES = 128
WORK = 5 * 10**9

norm_eps = 1e-05
clamp_limit = 7.0
glu_alpha = 1.702
highest = lax.Precision.HIGHEST
f32 = jnp.float32
bf16 = jnp.bfloat16


def clamped_unit(gate_pre, up_pre):
    glu_part = jnp.minimum(gate_pre, clamp_limit)
    lin_part = jnp.clip(up_pre, -clamp_limit, clamp_limit)
    return glu_part * jax.nn.sigmoid(glu_alpha * glu_part) * (lin_part + 1.0)


def state_step(
    inner_proj,
    gate_proj,
    write_proj,
    read_proj,
    step_raw,
    conv_state,
    conv_proj_state,
    conv_kernel,
    conv_proj_kernel,
    step_bias,
    log_rate,
    skip_gain,
    group_gain,
    head_state,
    group_count,
):
    window_inner = jnp.concatenate([conv_state, inner_proj[:, None, :]], axis=1)
    window_proj = jnp.concatenate(
        [conv_proj_state, jnp.stack([write_proj, read_proj], axis=1)[:, None]], axis=1
    )
    conv_inner = jax.nn.silu(jnp.sum(window_inner.astype(f32) * conv_kernel[None], axis=1))
    conv_proj = jax.nn.silu(jnp.sum(window_proj.astype(f32) * conv_proj_kernel[None], axis=1))
    seq_count, channels = conv_inner.shape
    head_count = step_raw.shape[1]
    head_width = channels // head_count
    state_width = conv_proj.shape[2] // group_count
    per_group = head_count // group_count
    head_input = conv_inner.reshape(seq_count, head_count, head_width)
    write_heads = jnp.repeat(
        conv_proj[:, 0].reshape(seq_count, group_count, state_width), per_group, axis=1
    )
    read_heads = jnp.repeat(
        conv_proj[:, 1].reshape(seq_count, group_count, state_width), per_group, axis=1
    )
    step_size = jax.nn.softplus(step_raw + step_bias)
    decay_rate = jnp.exp(-jnp.exp(log_rate) * step_size)
    state_out = (
        decay_rate[:, :, None, None] * head_state
        + (step_size[:, :, None] * head_input)[:, :, :, None] * write_heads[:, :, None, :]
    )
    read_out = (
        jnp.sum(state_out * read_heads[:, :, None, :], axis=-1)
        + skip_gain[None, :, None] * head_input
    )
    gated_rows = read_out.reshape(seq_count, channels) * jax.nn.silu(gate_proj.astype(f32))
    grouped = gated_rows.reshape(seq_count, group_count, channels // group_count)
    grouped = grouped * lax.rsqrt(jnp.mean(grouped * grouped, axis=-1, keepdims=True) + norm_eps)
    mixer_rows = (grouped.reshape(seq_count, channels) * group_gain).astype(bf16)
    return (mixer_rows, state_out, window_inner[:, 1:], window_proj[:, 1:])


def open_kernel(out_ref):
    out_ref[...] = jnp.zeros_like(out_ref)


def early_kernel(
    tokens_ref,
    gain_ref,
    write_ref,
    read_ref,
    step_ref,
    conv_state_ref,
    proj_state_ref,
    kernel_ref,
    proj_kernel_ref,
    bias_ref,
    rate_ref,
    skip_ref,
    group_gain_ref,
    routes_ref,
    logits_ref,
    state_ref,
    rows_ref,
    vec_ref,
    tail_ref,
    proj_out_ref,
    buf_ref,
    wait_state,
):
    taps = kernel_ref.shape[0]
    seq, width = tokens_ref.shape
    heads = bias_ref.shape[1]
    channels = kernel_ref.shape[1]
    head_width, state_width = state_ref.shape[2:]
    groups = write_ref.shape[1] // state_width
    per_group = heads // groups
    span = per_group * head_width
    blocks = channels // LANES

    tok = tokens_ref[...].astype(f32)
    scale = lax.rsqrt(jnp.sum(tok * tok, axis=1, keepdims=True) / width + norm_eps)
    normed = (tok * scale * gain_ref[...]).astype(bf16)
    write = jnp.dot(normed, write_ref[...], preferred_element_type=f32).astype(bf16)
    read = jnp.dot(normed, read_ref[...], preferred_element_type=f32).astype(bf16)
    step = lax.dot_general(
        normed, step_ref[...], (((1,), (1,)), ((), ())), preferred_element_type=f32
    )
    step = step + bias_ref[...]
    dt = jnp.maximum(step, 0.0) + jnp.log1p(jnp.exp(-jnp.abs(step)))
    decay = jnp.exp(-jnp.exp(rate_ref[...]) * dt)

    tail_ref[...] = jnp.zeros(tail_ref.shape, f32)
    top = routes_ref.shape[1]
    tail_ref[:, 0:top] = routes_ref[...].astype(f32)
    tail_ref[:, top : 2 * top] = logits_ref[...].astype(f32)

    for t in range(taps - 2):
        proj_out_ref[:, t] = proj_state_ref[:, t + 1]
    for t in range(seq):
        proj_out_ref[t, taps - 2, 0:1, :] = write[t : t + 1]
        proj_out_ref[t, taps - 2, 1:2, :] = read[t : t + 1]
        for i, new in ((0, write), (1, read)):
            total = new[t : t + 1].astype(f32) * proj_kernel_ref[taps - 1, i : i + 1, :]
            for j in range(taps - 1):
                total += (
                    proj_state_ref[t, j, i : i + 1, :].astype(f32)
                    * proj_kernel_ref[j, i : i + 1, :]
                )
            vec_ref[i, t : t + 1, :] = total * jax.nn.sigmoid(total)

    head = lax.broadcasted_iota(jnp.int32, (heads, channels), 0)
    chan = lax.broadcasted_iota(jnp.int32, (heads, channels), 1)
    spread = jnp.where(chan // head_width == head, 1.0, 0.0)

    def wide(v):
        return jnp.dot(v, spread, precision=highest, preferred_element_type=f32)

    dt_wide = wide(dt)
    decay_wide = wide(decay)
    skip_wide = wide(jnp.broadcast_to(skip_ref[...], (seq, heads)))

    def place(index, v):
        for c in range(blocks):
            rows_ref[index, c * seq : (c + 1) * seq, :] = v[:, c * LANES : (c + 1) * LANES]

    conv = jnp.zeros((seq, channels), f32)
    for j in range(taps - 1):
        conv += conv_state_ref[j].astype(f32) * kernel_ref[j : j + 1, :]
    place(0, conv)
    place(1, jnp.broadcast_to(kernel_ref[taps - 1 : taps, :], (seq, channels)))

    wait_state()
    for t in range(seq):
        for g in range(groups):
            cols = slice(g * state_width, (g + 1) * state_width)
            lanes = slice(g * span, (g + 1) * span)
            read_vec = vec_ref[1, t : t + 1, cols]
            read_hi = read_vec.astype(bf16)
            read_lo = (read_vec - read_hi.astype(f32)).astype(bf16)
            old = state_ref[t, g * per_group : (g + 1) * per_group].reshape(span, state_width)
            old_hi = old.astype(bf16)
            old_lo = (old - old_hi.astype(f32)).astype(bf16)

            def along(x, y):
                return lax.dot_general(
                    x, y, (((1,), (1,)), ((), ())), preferred_element_type=f32
                )

            sums = along(read_hi, old_hi) + along(read_hi, old_lo) + along(read_lo, old_hi)
            buf_ref[t : t + 1, lanes] = sums
            meet = jnp.sum(vec_ref[0, t : t + 1, cols] * read_vec, axis=1, keepdims=True)
            buf_ref[seq + t : seq + t + 1, lanes] = jnp.broadcast_to(meet, (1, span))
    place(2, decay_wide * buf_ref[0:seq, :])
    place(3, dt_wide * buf_ref[seq : 2 * seq, :] + skip_wide)
    place(4, jnp.broadcast_to(group_gain_ref[...], (seq, channels)))
    place(5, jnp.broadcast_to(scale, (seq, channels)))
    place(6, dt_wide)
    place(7, decay_wide)


def early_stage(count, *refs):
    sources, outs = refs[:count], refs[count + 1 : count + 5]
    buf_ref, state_ref, sems = refs[count + 5 :]
    copy = pltpu.make_async_copy(sources[-1], state_ref, sems.at[0])
    copy.start()
    early_kernel(*sources[:-1], state_ref, *outs, buf_ref, copy.wait)


def project_kernel(
    raw_ref, gain_ref, gate_ref, inner_ref, tail_ref, out_ref, tok_ref, in_ref, buf_ref
):
    count, rows, lanes = out_ref.shape
    seq = tail_ref.shape[0]
    blocks = gate_ref.shape[1] // lanes
    in_ref[...] = raw_ref[...].astype(f32)
    for t in range(seq):
        tok_ref[t * count : (t + 1) * count, :] = in_ref[pl.ds(t, count, stride=seq), :]
    gain = gain_ref[pl.ds(lax.axis_index("ep"), 1), :]
    x = (tok_ref[...] * gain).astype(bf16)
    for i, weight in ((0, gate_ref), (1, inner_ref)):
        y = jnp.dot(x, weight[...], preferred_element_type=f32)
        for c in range(blocks):
            for t in range(seq):
                buf_ref[pl.ds((i * blocks + c) * seq + t, count, stride=rows), :] = y[
                    t * count : (t + 1) * count, c * lanes : (c + 1) * lanes
                ]
    last = 2 * blocks * seq
    tail = jnp.concatenate([tail_ref[...], jnp.zeros((rows - last - seq, lanes), f32)], axis=0)
    for p in range(count):
        buf_ref[p * rows + last : (p + 1) * rows, :] = tail
        out_ref[p] = buf_ref[p * rows : (p + 1) * rows, :].astype(bf16)


def mixer_kernel(seq, terms_ref, pre_ref, out_ref, conv_ref, inner_ref, tail_ref, buf_ref):
    count, _, lanes = terms_ref.shape
    n_all, blocks, _ = out_ref.shape
    half = blocks * seq
    total = jnp.zeros((2 * half, lanes), f32)
    for p in range(count):
        total += terms_ref[p, 0 : 2 * half, :].astype(f32)
        buf_ref[p * 8 : (p + 1) * 8, :] = terms_ref[p, 2 * half : 2 * half + 8, :].astype(f32)
    for t in range(seq):
        tail_ref[t * count : (t + 1) * count, :] = buf_ref[pl.ds(t, count, stride=8), :]
    scale = pre_ref[5]
    gate = (total[0:half] * scale).astype(bf16).astype(f32)
    inner = (total[half : 2 * half] * scale).astype(bf16).astype(f32)
    conv = pre_ref[0] + pre_ref[1] * inner
    conv = conv * jax.nn.sigmoid(conv)
    conv_ref[...] = conv
    inner_ref[...] = inner
    gated = (pre_ref[2] + pre_ref[3] * conv) * (gate * jax.nn.sigmoid(gate))
    groups = GROUPS // lax.axis_size("tp")
    span = half // groups
    for g in range(groups):
        part = gated[g * span : (g + 1) * span]
        square = jnp.sum(part * part, axis=1, keepdims=True)
        square = jnp.broadcast_to(square, (span, lanes))
        whole = square
        for k in range(1, span // seq):
            whole += pltpu.roll(square, k * seq, 0)
        part = part * lax.rsqrt(whole / (span // seq * lanes) + norm_eps)
        buf_ref[g * span : (g + 1) * span, :] = part * pre_ref[4, g * span : (g + 1) * span, :]
    for t in range(seq):
        mixed = buf_ref[pl.ds(t, blocks, stride=seq), :].astype(bf16)
        for d in range(t, n_all, seq):
            out_ref[d] = mixed


def hidden_kernel(
    count, mix_ref, own_ref, other_ref, tok_ref, out_ref, buf_ref, lhs_ref
):
    n_all, blocks, lanes = mix_ref.shape
    n_tp = n_all // count
    my_tp = lax.axis_index("tp")
    for d in range(n_all):
        buf_ref[d * blocks : (d + 1) * blocks, :] = mix_ref[d].astype(f32)
    total = tok_ref[pl.ds(pl.multiple_of(my_tp * count, count), count), :]
    for which, weight in ((0, own_ref), (1, other_ref)):
        core = lax.rem(my_tp + which, n_tp)
        for c in range(blocks):
            lhs_ref[:, c * lanes : (c + 1) * lanes] = buf_ref[
                pl.ds(core * blocks + c, count, stride=n_tp * blocks), :
            ].astype(bf16)
        total += jnp.dot(lhs_ref[...], weight[...], preferred_element_type=f32)
    hidden = total.astype(bf16)
    for d in range(n_all):
        out_ref[d] = hidden


def new_states(
    state_ref,
    conv_ref,
    inner_ref,
    pre_ref,
    vec_ref,
    old_ref,
    state_out_ref,
    conv_out_ref,
    new_ref,
    taps_ref,
    sems,
):
    seq, heads, head_width, state_width = state_ref.shape
    half, lanes = conv_ref.shape
    taps = taps_ref.shape[0]
    groups = vec_ref.shape[2] // state_width
    per_group = heads // groups
    per_block = lanes // head_width
    columns = jnp.concatenate([pre_ref[6] * conv_ref[...], pre_ref[7]], axis=0).T
    copies = []
    for t in range(seq):
        for h in range(heads):
            row = h // per_block * seq + t
            part = slice(h % per_block * head_width, (h % per_block + 1) * head_width)
            g = h // per_group
            write = vec_ref[0, t : t + 1, g * state_width : (g + 1) * state_width]
            new_ref[t, h] = (
                columns[part, half + row : half + row + 1] * state_ref[t, h]
                + columns[part, row : row + 1] * write
            )
        copies.append(
            pltpu.make_async_copy(new_ref.at[t], state_out_ref.at[t], sems.at[t])
        )
        copies[-1].start()
    for j in range(taps - 1):
        taps_ref[j] = old_ref[j + 1]
    for c in range(half // seq):
        taps_ref[taps - 1, :, c * lanes : (c + 1) * lanes] = inner_ref[
            c * seq : (c + 1) * seq, :
        ].astype(bf16)
    copies.append(pltpu.make_async_copy(taps_ref, conv_out_ref, sems.at[seq]))
    copies[-1].start()
    return copies


def expert_kernel(
    top,
    seq,
    hid_ref,
    tail_ref,
    gain_ref,
    dgate_ref,
    gate_ref,
    up_ref,
    down_ref,
    dup_ref,
    ddown_ref,
    state_ref,
    conv_ref,
    inner_ref,
    pre_ref,
    vec_ref,
    old_ref,
    out_ref,
    own_ref,
    state_out_ref,
    conv_out_ref,
    x_ref,
    h_ref,
    t_ref,
    new_ref,
    taps_ref,
    sems,
):
    copies = new_states(
        state_ref,
        conv_ref,
        inner_ref,
        pre_ref,
        vec_ref,
        old_ref,
        state_out_ref,
        conv_out_ref,
        new_ref,
        taps_ref,
        sems,
    )
    count, lanes = hid_ref.shape[1:]
    rows = count * seq
    blocks = hid_ref.shape[0] // seq
    my_ep = lax.axis_index("ep")
    own = lax.axis_index("tp") * count + my_ep
    total = jnp.zeros((rows, lanes), f32)
    for k in range(blocks):
        for t in range(seq):
            at = k * rows + t * count
            h_ref[at : at + count, :] = hid_ref[k * seq + t].astype(f32)
        h = h_ref[k * rows : (k + 1) * rows, :]
        total += h * h
    scale = lax.rsqrt(jnp.sum(total, axis=1, keepdims=True) / (blocks * lanes) + norm_eps)
    dense = jnp.zeros((rows, lanes), f32)
    for k in range(blocks):
        h = h_ref[k * rows : (k + 1) * rows, :]
        x = (h * scale * gain_ref[k : k + 1, :]).astype(bf16)
        x_ref[:, k * lanes : (k + 1) * lanes] = x
        dense += x.astype(f32) * dgate_ref[k : k + 1, :]
    own_ref[...] = h_ref[pl.ds(own, blocks, stride=rows), :]
    dense_weight = jax.nn.sigmoid(jnp.sum(dense, axis=1, keepdims=True))

    tail = tail_ref[...]
    lane = lax.broadcasted_iota(jnp.int32, tail.shape, 1)
    scored = (lane >= top) & (lane < 2 * top)
    peak = jnp.max(jnp.where(scored, tail, -3e38), axis=1, keepdims=True)
    raised = jnp.where(scored, jnp.exp(jnp.minimum(tail - peak, 0.0)), 0.0)
    hits = (lane < top) & (tail.astype(jnp.int32) == my_ep)
    picked = jnp.where(hits, pltpu.roll(raised, lanes - top, 1), 0.0)
    row_weight = jnp.sum(picked, axis=1, keepdims=True) / jnp.sum(raised, axis=1, keepdims=True)

    x = x_ref[...]
    gate = jnp.dot(x, gate_ref[...], preferred_element_type=f32)
    up = jnp.dot(x, up_ref[...], preferred_element_type=f32)
    act = (clamped_unit(gate, up) * row_weight).astype(bf16)
    inner = jnp.dot(x, dup_ref[...], preferred_element_type=f32)
    dact = (inner * jax.nn.sigmoid(inner) * dense_weight).astype(bf16)
    wide = 4
    for j in range(blocks // wide):
        cols = slice(j * wide * lanes, (j + 1) * wide * lanes)
        y = jnp.dot(act, down_ref[:, cols], preferred_element_type=f32) + jnp.dot(
            dact, ddown_ref[:, cols], preferred_element_type=f32
        )
        for i in range(wide):
            for t in range(seq):
                t_ref[pl.ds(t * blocks + j * wide + i, count, stride=seq * blocks), :] = y[
                    t * count : (t + 1) * count, i * lanes : (i + 1) * lanes
                ]
    for r in range(rows):
        out_ref[r] = t_ref[r * blocks : (r + 1) * blocks, :].astype(bf16)
    for copy in copies:
        copy.wait()


def call(kernel, outs, args, scratch, limit, anywhere=(), sems=0, work=None, outside=()):
    vmem = pl.BlockSpec(memory_space=pltpu.VMEM)
    hbm = pl.BlockSpec(memory_space=pltpu.HBM)
    args = [
        pltpu.with_memory_space_constraint(v, pltpu.HBM) if i in anywhere else v
        for i, v in enumerate(args)
    ]
    return pl.pallas_call(
        kernel,
        out_shape=tuple(jax.ShapeDtypeStruct(shape, kind) for shape, kind in outs),
        in_specs=[hbm if i in anywhere else vmem for i in range(len(args))],
        out_specs=tuple(hbm if i in outside else vmem for i in range(len(outs))),
        scratch_shapes=[pltpu.VMEM(shape, kind) for shape, kind in scratch]
        + ([pltpu.SemaphoreType.DMA((sems,))] if sems else []),
        cost_estimate=work and pl.CostEstimate(
            flops=work, bytes_accessed=2**20, transcendentals=0
        ),
        compiler_params=pltpu.CompilerParams(vmem_limit_bytes=limit * 2**20),
    )(*args)


def final_kernel(terms_ref, own_ref, out_ref):
    count, blocks, lanes = terms_ref.shape
    total = own_ref[...]
    for r in range(count):
        total += terms_ref[r].astype(f32)
    for k in range(blocks):
        out_ref[:, k * lanes : (k + 1) * lanes] = total[k : k + 1, :].astype(bf16)


def final_stage(terms, own):
    _, blocks, lanes = terms.shape
    vmem = pl.BlockSpec(memory_space=pltpu.VMEM)
    return pl.pallas_call(
        final_kernel,
        name="final_stage",
        out_shape=jax.ShapeDtypeStruct((1, blocks * lanes), bf16),
        in_specs=[vmem] * 2,
        out_specs=vmem,
        compiler_params=pltpu.CompilerParams(vmem_limit_bytes=4 * 2**20),
    )(terms, own)


def direct(
    tokens,
    head_state,
    conv_state,
    conv_proj_state,
    first_gain,
    gate_weight,
    inner_weight,
    write_weight,
    read_weight,
    step_weight,
    conv_kernel,
    conv_proj_kernel,
    step_bias,
    log_rate,
    skip_gain,
    group_gain,
    out_weight,
    second_gain,
    routes,
    route_logits,
    expert_gate,
    expert_up,
    expert_down,
    dense_up,
    dense_down,
    dense_gate,
):
    n_ep = lax.axis_size("ep")
    n_tp = lax.axis_size("tp")
    n_all = n_ep * n_tp
    seq, width = tokens.shape
    rows = seq * n_ep
    channels = gate_weight.shape[1]
    half = channels // LANES * seq
    heads = step_weight.shape[1]
    state_cols = write_weight.shape[1]
    top = routes.shape[1]

    raw = lax.all_to_all(tokens, "ep", split_axis=1, concat_axis=0, tiled=True)

    swap = [(i, (i + 1) % n_tp) for i in range(n_tp)]
    other_weight = lax.ppermute(out_weight, "tp", swap)

    operands = (
        tokens,
        first_gain.reshape(1, width),
        write_weight,
        read_weight,
        step_weight.T,
        conv_state.transpose(1, 0, 2),
        conv_proj_state,
        conv_kernel,
        conv_proj_kernel,
        step_bias.reshape(1, heads),
        log_rate.reshape(1, heads),
        skip_gain.reshape(1, heads),
        group_gain.reshape(1, channels),
        routes,
        route_logits,
        head_state,
    )
    (opened,) = call(open_kernel, (((8, LANES), f32),), (), (), 1, work=WORK)
    early, vectors, tail, proj_out = call(
        functools.partial(early_stage, len(operands)),
        (
            ((8, half, LANES), f32),
            ((2, seq, state_cols), f32),
            ((seq, LANES), f32),
            (conv_proj_state.shape, bf16),
        ),
        (*operands, opened),
        (((2 * seq, channels), f32), (head_state.shape, f32)),
        6,
        (len(operands) - 1,),
        1,
    )

    raw, other_weight = lax.optimization_barrier((raw, other_weight))
    terms, tok_block = call(
        project_kernel,
        (((n_ep, 2 * half + 8, LANES), bf16), ((rows, LANES), f32)),
        (raw, first_gain.reshape(n_ep, LANES), gate_weight, inner_weight, tail),
        (((rows, LANES), f32), ((n_ep * (2 * half + 8), LANES), f32)),
        6,
        work=WORK,
    )
    terms = lax.all_to_all(terms, "ep", split_axis=0, concat_axis=0, tiled=True)

    mixed, conv, inner, tails = call(
        functools.partial(mixer_kernel, seq),
        (
            ((n_all, half // seq, LANES), bf16),
            ((half, LANES), f32),
            ((half, LANES), f32),
            ((rows, LANES), f32),
        ),
        (terms, early),
        (((max(n_ep * 8, half), LANES), f32),),
        4,
        work=WORK,
    )
    mixed = lax.all_to_all(mixed, ("ep", "tp"), split_axis=0, concat_axis=0, tiled=True)

    (hidden,) = call(
        functools.partial(hidden_kernel, n_ep),
        (((n_all, n_ep, LANES), bf16),),
        (mixed, out_weight, other_weight, tok_block),
        (((n_all * half // seq, LANES), f32), ((n_ep, channels), bf16)),
        6,
        work=WORK,
    )
    hidden = lax.all_to_all(hidden, ("ep", "tp"), split_axis=0, concat_axis=0, tiled=True)

    old = conv_state.transpose(1, 0, 2)
    terms, own_row, state_out, conv_out = call(
        functools.partial(expert_kernel, top, seq),
        (
            ((rows, n_ep, LANES), bf16),
            ((n_ep, LANES), f32),
            (head_state.shape, f32),
            (old.shape, bf16),
        ),
        (
            hidden,
            tails,
            second_gain.reshape(n_ep, LANES),
            dense_gate.reshape(n_ep, LANES),
            expert_gate[0],
            expert_up[0],
            expert_down[0],
            dense_up,
            dense_down,
            head_state,
            conv,
            inner,
            early,
            vectors,
            old,
        ),
        (
            ((rows, width), bf16),
            ((rows * n_ep, LANES), f32),
            ((rows * n_ep, LANES), f32),
            (head_state.shape, f32),
            (old.shape, bf16),
        ),
        8,
        sems=seq + 1,
        outside=(2, 3),
    )
    terms = lax.all_to_all(terms, ("ep", "tp"), split_axis=0, concat_axis=0, tiled=True)
    conv_out = conv_out.transpose(1, 0, 2)
    layer_out = final_stage(terms, own_row)
    return (layer_out, state_out, conv_out, proj_out)


def local(
    tokens,
    head_state,
    conv_state,
    conv_proj_state,
    first_gain,
    gate_weight,
    inner_weight,
    write_weight,
    read_weight,
    step_weight,
    conv_kernel,
    conv_proj_kernel,
    step_bias,
    log_rate,
    skip_gain,
    group_gain,
    out_weight,
    second_gain,
    routes,
    route_logits,
    expert_gate,
    expert_up,
    expert_down,
    dense_up,
    dense_down,
    dense_gate,
):
    n_ep = lax.axis_size("ep")
    n_tp = lax.axis_size("tp")
    n_all = n_ep * n_tp
    my_ep = lax.axis_index("ep")
    my_tp = lax.axis_index("tp")
    seq, width = tokens.shape
    rows = seq * n_ep
    half = gate_weight.shape[1]
    block = gate_weight.shape[0]

    if block == LANES and n_all == rows and seq == n_tp and half % LANES == 0:
        return direct(
            tokens,
            head_state,
            conv_state,
            conv_proj_state,
            first_gain,
            gate_weight,
            inner_weight,
            write_weight,
            read_weight,
            step_weight,
            conv_kernel,
            conv_proj_kernel,
            step_bias,
            log_rate,
            skip_gain,
            group_gain,
            out_weight,
            second_gain,
            routes,
            route_logits,
            expert_gate,
            expert_up,
            expert_down,
            dense_up,
            dense_down,
            dense_gate,
        )

    raw_block = lax.all_to_all(tokens, "ep", split_axis=1, concat_axis=0, tiled=True)

    tok = tokens.astype(f32)
    scale = lax.rsqrt(jnp.mean(tok * tok, axis=-1, keepdims=True) + norm_eps)
    normed_in = (tok * scale * first_gain).astype(bf16)
    write_proj = jnp.dot(normed_in, write_weight, preferred_element_type=f32).astype(bf16)
    read_proj = jnp.dot(normed_in, read_weight, preferred_element_type=f32).astype(bf16)
    step_raw = jnp.dot(normed_in, step_weight, preferred_element_type=f32)

    swap = [(i, (i + 1) % n_tp) for i in range(n_tp)]
    other_weight = lax.ppermute(out_weight, "tp", swap)

    gain_block = lax.dynamic_slice_in_dim(first_gain, my_ep * block, block, 0)
    scaled = (raw_block.astype(f32) * gain_block).astype(bf16)
    terms = jnp.concatenate(
        [
            jnp.dot(scaled, gate_weight, preferred_element_type=f32).astype(bf16),
            jnp.dot(scaled, inner_weight, preferred_element_type=f32).astype(bf16),
        ],
        axis=1,
    ).reshape(n_ep, seq, 2 * half)
    terms = lax.all_to_all(terms, "ep", split_axis=0, concat_axis=0, tiled=True)
    both = jnp.sum(terms.astype(f32), axis=0) * scale
    gate_proj = both[:, :half].astype(bf16)
    inner_proj = both[:, half:].astype(bf16)

    mixer_rows, state_out, conv_out, conv_proj_out = state_step(
        inner_proj,
        gate_proj,
        write_proj,
        read_proj,
        step_raw,
        conv_state,
        conv_proj_state,
        conv_kernel,
        conv_proj_kernel,
        step_bias,
        log_rate,
        skip_gain,
        group_gain,
        head_state,
        GROUPS // n_tp,
    )

    top = routes.shape[1]
    tail = jnp.concatenate(
        [routes.astype(bf16), route_logits, jnp.zeros((seq, TAIL - 2 * top), bf16)], axis=1
    )
    packed = jnp.concatenate([mixer_rows, tail], axis=1)
    packed = jnp.broadcast_to(packed[None], (n_all, seq, half + TAIL))
    packed = lax.all_to_all(packed, ("ep", "tp"), split_axis=0, concat_axis=0, tiled=True)
    packed = packed.reshape(n_ep, n_tp, seq, half + TAIL)
    own_half = lax.dynamic_index_in_dim(packed, my_tp, 1, keepdims=False)
    other_half = lax.dynamic_index_in_dim(packed, n_tp - 1 - my_tp, 1, keepdims=False)
    own_half = own_half.reshape(rows, half + TAIL)
    other_half = other_half.reshape(rows, half + TAIL)
    all_routes = own_half[:, half : half + top]
    all_logits = own_half[:, half + top : half + 2 * top]
    mixed = jnp.dot(own_half[:, :half], out_weight, preferred_element_type=f32) + jnp.dot(
        other_half[:, :half], other_weight, preferred_element_type=f32
    )
    hidden_block = (raw_block.astype(f32) + mixed).astype(bf16)

    hidden = jnp.broadcast_to(hidden_block[None], (n_ep, rows, block))
    hidden = lax.all_to_all(hidden, "ep", split_axis=0, concat_axis=0, tiled=True)
    hidden = hidden.transpose(1, 0, 2).reshape(rows, width)

    hid = hidden.astype(f32)
    normed = hid * lax.rsqrt(jnp.mean(hid * hid, axis=-1, keepdims=True) + norm_eps) * second_gain
    normed_mid = normed.astype(bf16)

    route_gates = jax.nn.softmax(all_logits.astype(f32), axis=-1)
    row_weight = jnp.sum(
        jnp.where(all_routes.astype(jnp.int32) == my_ep, route_gates, 0.0), axis=1, keepdims=True
    )
    dense_weight = jax.nn.sigmoid(
        jnp.sum(normed_mid.astype(f32) * dense_gate, axis=-1, keepdims=True)
    )
    activated = clamped_unit(
        jnp.dot(normed_mid, expert_gate[0], preferred_element_type=f32),
        jnp.dot(normed_mid, expert_up[0], preferred_element_type=f32),
    ).astype(bf16)
    dense_inner = jax.nn.silu(
        jnp.dot(normed_mid, dense_up, preferred_element_type=f32)
    ).astype(bf16)
    total = (
        jnp.dot(activated, expert_down[0], preferred_element_type=f32) * row_weight
        + jnp.dot(dense_inner, dense_down, preferred_element_type=f32) * dense_weight
    ).astype(bf16)

    row_share = rows // n_all
    total = total.reshape(n_all, row_share, width)
    total = lax.all_to_all(total, ("ep", "tp"), split_axis=0, concat_axis=0, tiled=True)
    summed = jnp.sum(total.astype(f32), axis=0)
    own_rows = lax.dynamic_slice_in_dim(
        hidden, (my_ep * n_tp + my_tp) * row_share, row_share, 0
    )
    layer_out = (own_rows.astype(f32) + summed).astype(bf16)
    return (layer_out, state_out, conv_out, conv_proj_out)


def solution(mesh):
    placed = (
        P("ep", None),
        P("ep", "tp", None, None),
        P("ep", None, "tp"),
        P("ep", None, None, "tp"),
        P(),
        P("ep", "tp"),
        P("ep", "tp"),
        P(None, "tp"),
        P(None, "tp"),
        P(None, "tp"),
        P(None, "tp"),
        P(None, None, "tp"),
        P("tp"),
        P("tp"),
        P("tp"),
        P("tp"),
        P("tp", "ep"),
        P(),
        P("ep", None),
        P("ep", None),
        P("ep", None, "tp"),
        P("ep", None, "tp"),
        P("ep", "tp", None),
        P(None, ("ep", "tp")),
        P(("ep", "tp"), None),
        P(),
    )
    return jax.shard_map(
        local,
        mesh=mesh,
        in_specs=placed,
        out_specs=(
            P(("ep", "tp"), None),
            P("ep", "tp", None, None),
            P("ep", None, "tp"),
            P("ep", None, None, "tp"),
        ),
        check_vma=False,
    )
```

```python
import functools

import jax
import jax.numpy as jnp
from jax import lax
from jax.experimental import pallas as pl
from jax.experimental.pallas import tpu as pltpu
from jax.sharding import PartitionSpec as P

GROUPS = 4
TAIL = 128
LANES = 128
WORK = 5 * 10**9

norm_eps = 1e-05
clamp_limit = 7.0
glu_alpha = 1.702
highest = lax.Precision.HIGHEST
f32 = jnp.float32
bf16 = jnp.bfloat16


def clamped_unit(gate_pre, up_pre):
    glu_part = jnp.minimum(gate_pre, clamp_limit)
    lin_part = jnp.clip(up_pre, -clamp_limit, clamp_limit)
    return glu_part * jax.nn.sigmoid(glu_alpha * glu_part) * (lin_part + 1.0)


def state_step(
    inner_proj,
    gate_proj,
    write_proj,
    read_proj,
    step_raw,
    conv_state,
    conv_proj_state,
    conv_kernel,
    conv_proj_kernel,
    step_bias,
    log_rate,
    skip_gain,
    group_gain,
    head_state,
    group_count,
):
    window_inner = jnp.concatenate([conv_state, inner_proj[:, None, :]], axis=1)
    window_proj = jnp.concatenate(
        [conv_proj_state, jnp.stack([write_proj, read_proj], axis=1)[:, None]], axis=1
    )
    conv_inner = jax.nn.silu(jnp.sum(window_inner.astype(f32) * conv_kernel[None], axis=1))
    conv_proj = jax.nn.silu(jnp.sum(window_proj.astype(f32) * conv_proj_kernel[None], axis=1))
    seq_count, channels = conv_inner.shape
    head_count = step_raw.shape[1]
    head_width = channels // head_count
    state_width = conv_proj.shape[2] // group_count
    per_group = head_count // group_count
    head_input = conv_inner.reshape(seq_count, head_count, head_width)
    write_heads = jnp.repeat(
        conv_proj[:, 0].reshape(seq_count, group_count, state_width), per_group, axis=1
    )
    read_heads = jnp.repeat(
        conv_proj[:, 1].reshape(seq_count, group_count, state_width), per_group, axis=1
    )
    step_size = jax.nn.softplus(step_raw + step_bias)
    decay_rate = jnp.exp(-jnp.exp(log_rate) * step_size)
    state_out = (
        decay_rate[:, :, None, None] * head_state
        + (step_size[:, :, None] * head_input)[:, :, :, None] * write_heads[:, :, None, :]
    )
    read_out = (
        jnp.sum(state_out * read_heads[:, :, None, :], axis=-1)
        + skip_gain[None, :, None] * head_input
    )
    gated_rows = read_out.reshape(seq_count, channels) * jax.nn.silu(gate_proj.astype(f32))
    grouped = gated_rows.reshape(seq_count, group_count, channels // group_count)
    grouped = grouped * lax.rsqrt(jnp.mean(grouped * grouped, axis=-1, keepdims=True) + norm_eps)
    mixer_rows = (grouped.reshape(seq_count, channels) * group_gain).astype(bf16)
    return (mixer_rows, state_out, window_inner[:, 1:], window_proj[:, 1:])


def open_kernel(out_ref):
    out_ref[...] = jnp.zeros_like(out_ref)


def early_kernel(
    tokens_ref,
    gain_ref,
    write_ref,
    read_ref,
    step_ref,
    conv_state_ref,
    proj_state_ref,
    kernel_ref,
    proj_kernel_ref,
    bias_ref,
    rate_ref,
    skip_ref,
    group_gain_ref,
    routes_ref,
    logits_ref,
    state_ref,
    rows_ref,
    vec_ref,
    tail_ref,
    proj_out_ref,
    buf_ref,
    wait_state,
):
    taps = kernel_ref.shape[0]
    seq, width = tokens_ref.shape
    heads = bias_ref.shape[1]
    channels = kernel_ref.shape[1]
    head_width, state_width = state_ref.shape[2:]
    groups = write_ref.shape[1] // state_width
    per_group = heads // groups
    span = per_group * head_width
    blocks = channels // LANES

    tok = tokens_ref[...].astype(f32)
    scale = lax.rsqrt(jnp.sum(tok * tok, axis=1, keepdims=True) / width + norm_eps)
    normed = (tok * scale * gain_ref[...]).astype(bf16)
    write = jnp.dot(normed, write_ref[...], preferred_element_type=f32).astype(bf16)
    read = jnp.dot(normed, read_ref[...], preferred_element_type=f32).astype(bf16)
    step = lax.dot_general(
        normed, step_ref[...], (((1,), (1,)), ((), ())), preferred_element_type=f32
    )
    step = step + bias_ref[...]
    dt = jnp.maximum(step, 0.0) + jnp.log1p(jnp.exp(-jnp.abs(step)))
    decay = jnp.exp(-jnp.exp(rate_ref[...]) * dt)

    tail_ref[...] = jnp.zeros(tail_ref.shape, f32)
    top = routes_ref.shape[1]
    tail_ref[:, 0:top] = routes_ref[...].astype(f32)
    tail_ref[:, top : 2 * top] = logits_ref[...].astype(f32)

    for t in range(taps - 2):
        proj_out_ref[:, t] = proj_state_ref[:, t + 1]
    for t in range(seq):
        proj_out_ref[t, taps - 2, 0:1, :] = write[t : t + 1]
        proj_out_ref[t, taps - 2, 1:2, :] = read[t : t + 1]
        for i, new in ((0, write), (1, read)):
            total = new[t : t + 1].astype(f32) * proj_kernel_ref[taps - 1, i : i + 1, :]
            for j in range(taps - 1):
                total += (
                    proj_state_ref[t, j, i : i + 1, :].astype(f32)
                    * proj_kernel_ref[j, i : i + 1, :]
                )
            vec_ref[i, t : t + 1, :] = total * jax.nn.sigmoid(total)

    head = lax.broadcasted_iota(jnp.int32, (heads, channels), 0)
    chan = lax.broadcasted_iota(jnp.int32, (heads, channels), 1)
    spread = jnp.where(chan // head_width == head, 1.0, 0.0)

    def wide(v):
        return jnp.dot(v, spread, precision=highest, preferred_element_type=f32)

    dt_wide = wide(dt)
    decay_wide = wide(decay)
    skip_wide = wide(jnp.broadcast_to(skip_ref[...], (seq, heads)))

    def place(index, v):
        for c in range(blocks):
            rows_ref[index, c * seq : (c + 1) * seq, :] = v[:, c * LANES : (c + 1) * LANES]

    conv = jnp.zeros((seq, channels), f32)
    for j in range(taps - 1):
        conv += conv_state_ref[j].astype(f32) * kernel_ref[j : j + 1, :]
    place(0, conv)
    place(1, jnp.broadcast_to(kernel_ref[taps - 1 : taps, :], (seq, channels)))

    wait_state()
    for t in range(seq):
        for g in range(groups):
            cols = slice(g * state_width, (g + 1) * state_width)
            lanes = slice(g * span, (g + 1) * span)
            read_vec = vec_ref[1, t : t + 1, cols]
            read_hi = read_vec.astype(bf16)
            read_lo = (read_vec - read_hi.astype(f32)).astype(bf16)
            old = state_ref[t, g * per_group : (g + 1) * per_group].reshape(span, state_width)
            old_hi = old.astype(bf16)
            old_lo = (old - old_hi.astype(f32)).astype(bf16)

            def along(x, y):
                return lax.dot_general(
                    x, y, (((1,), (1,)), ((), ())), preferred_element_type=f32
                )

            sums = along(read_hi, old_hi) + along(read_hi, old_lo) + along(read_lo, old_hi)
            buf_ref[t : t + 1, lanes] = sums
            meet = jnp.sum(vec_ref[0, t : t + 1, cols] * read_vec, axis=1, keepdims=True)
            buf_ref[seq + t : seq + t + 1, lanes] = jnp.broadcast_to(meet, (1, span))
    place(2, decay_wide * buf_ref[0:seq, :])
    place(3, dt_wide * buf_ref[seq : 2 * seq, :] + skip_wide)
    place(4, jnp.broadcast_to(group_gain_ref[...], (seq, channels)))
    place(5, jnp.broadcast_to(scale, (seq, channels)))
    place(6, dt_wide)
    place(7, decay_wide)


def early_stage(count, *refs):
    sources, outs = refs[:count], refs[count + 1 : count + 5]
    buf_ref, state_ref, sems = refs[count + 5 :]
    copy = pltpu.make_async_copy(sources[-1], state_ref, sems.at[0])
    copy.start()
    early_kernel(*sources[:-1], state_ref, *outs, buf_ref, copy.wait)


def project_kernel(
    raw_ref, gain_ref, gate_ref, inner_ref, tail_ref, out_ref, tok_ref, in_ref, buf_ref
):
    count, rows, lanes = out_ref.shape
    seq = tail_ref.shape[0]
    blocks = gate_ref.shape[1] // lanes
    in_ref[...] = raw_ref[...].astype(f32)
    for t in range(seq):
        tok_ref[t * count : (t + 1) * count, :] = in_ref[pl.ds(t, count, stride=seq), :]
    gain = gain_ref[pl.ds(lax.axis_index("ep"), 1), :]
    x = (tok_ref[...] * gain).astype(bf16)
    for i, weight in ((0, gate_ref), (1, inner_ref)):
        y = jnp.dot(x, weight[...], preferred_element_type=f32)
        for c in range(blocks):
            for t in range(seq):
                buf_ref[pl.ds((i * blocks + c) * seq + t, count, stride=rows), :] = y[
                    t * count : (t + 1) * count, c * lanes : (c + 1) * lanes
                ]
    last = 2 * blocks * seq
    tail = jnp.concatenate([tail_ref[...], jnp.zeros((rows - last - seq, lanes), f32)], axis=0)
    for p in range(count):
        buf_ref[p * rows + last : (p + 1) * rows, :] = tail
        out_ref[p] = buf_ref[p * rows : (p + 1) * rows, :].astype(bf16)


def mixer_kernel(seq, terms_ref, pre_ref, out_ref, conv_ref, inner_ref, tail_ref, buf_ref):
    count, _, lanes = terms_ref.shape
    n_all, blocks, _ = out_ref.shape
    half = blocks * seq
    total = jnp.zeros((2 * half, lanes), f32)
    for p in range(count):
        total += terms_ref[p, 0 : 2 * half, :].astype(f32)
        buf_ref[p * 8 : (p + 1) * 8, :] = terms_ref[p, 2 * half : 2 * half + 8, :].astype(f32)
    for t in range(seq):
        tail_ref[t * count : (t + 1) * count, :] = buf_ref[pl.ds(t, count, stride=8), :]
    scale = pre_ref[5]
    gate = (total[0:half] * scale).astype(bf16).astype(f32)
    inner = (total[half : 2 * half] * scale).astype(bf16).astype(f32)
    conv = pre_ref[0] + pre_ref[1] * inner
    conv = conv * jax.nn.sigmoid(conv)
    conv_ref[...] = conv
    inner_ref[...] = inner
    gated = (pre_ref[2] + pre_ref[3] * conv) * (gate * jax.nn.sigmoid(gate))
    groups = GROUPS // lax.axis_size("tp")
    span = half // groups
    for g in range(groups):
        part = gated[g * span : (g + 1) * span]
        square = jnp.sum(part * part, axis=1, keepdims=True)
        square = jnp.broadcast_to(square, (span, lanes))
        whole = square
        for k in range(1, span // seq):
            whole += pltpu.roll(square, k * seq, 0)
        part = part * lax.rsqrt(whole / (span // seq * lanes) + norm_eps)
        buf_ref[g * span : (g + 1) * span, :] = part * pre_ref[4, g * span : (g + 1) * span, :]
    for t in range(seq):
        mixed = buf_ref[pl.ds(t, blocks, stride=seq), :].astype(bf16)
        for d in range(t, n_all, seq):
            out_ref[d] = mixed


def hidden_kernel(
    count, mix_ref, own_ref, other_ref, tok_ref, out_ref, buf_ref, lhs_ref
):
    n_all, blocks, lanes = mix_ref.shape
    n_tp = n_all // count
    my_tp = lax.axis_index("tp")
    for d in range(n_all):
        buf_ref[d * blocks : (d + 1) * blocks, :] = mix_ref[d].astype(f32)
    total = tok_ref[pl.ds(pl.multiple_of(my_tp * count, count), count), :]
    for which, weight in ((0, own_ref), (1, other_ref)):
        core = lax.rem(my_tp + which, n_tp)
        for c in range(blocks):
            lhs_ref[:, c * lanes : (c + 1) * lanes] = buf_ref[
                pl.ds(core * blocks + c, count, stride=n_tp * blocks), :
            ].astype(bf16)
        total += jnp.dot(lhs_ref[...], weight[...], preferred_element_type=f32)
    hidden = total.astype(bf16)
    for d in range(n_all):
        out_ref[d] = hidden


def new_states(
    state_ref,
    conv_ref,
    inner_ref,
    pre_ref,
    vec_ref,
    old_ref,
    state_out_ref,
    conv_out_ref,
    new_ref,
    taps_ref,
    sems,
):
    seq, heads, head_width, state_width = state_ref.shape
    half, lanes = conv_ref.shape
    taps = taps_ref.shape[0]
    groups = vec_ref.shape[2] // state_width
    per_group = heads // groups
    per_block = lanes // head_width
    columns = jnp.concatenate([pre_ref[6] * conv_ref[...], pre_ref[7]], axis=0).T
    copies = []
    for t in range(seq):
        for h in range(heads):
            row = h // per_block * seq + t
            part = slice(h % per_block * head_width, (h % per_block + 1) * head_width)
            g = h // per_group
            write = vec_ref[0, t : t + 1, g * state_width : (g + 1) * state_width]
            new_ref[t, h] = (
                columns[part, half + row : half + row + 1] * state_ref[t, h]
                + columns[part, row : row + 1] * write
            )
        copies.append(
            pltpu.make_async_copy(new_ref.at[t], state_out_ref.at[t], sems.at[t])
        )
        copies[-1].start()
    for j in range(taps - 1):
        taps_ref[j] = old_ref[j + 1]
    for c in range(half // seq):
        taps_ref[taps - 1, :, c * lanes : (c + 1) * lanes] = inner_ref[
            c * seq : (c + 1) * seq, :
        ].astype(bf16)
    copies.append(pltpu.make_async_copy(taps_ref, conv_out_ref, sems.at[seq]))
    copies[-1].start()
    return copies


def expert_kernel(
    top,
    seq,
    hid_ref,
    tail_ref,
    gain_ref,
    dgate_ref,
    gate_ref,
    up_ref,
    down_ref,
    dup_ref,
    ddown_ref,
    state_ref,
    conv_ref,
    inner_ref,
    pre_ref,
    vec_ref,
    old_ref,
    out_ref,
    own_ref,
    state_out_ref,
    conv_out_ref,
    x_ref,
    h_ref,
    t_ref,
    new_ref,
    taps_ref,
    sems,
):
    count, lanes = hid_ref.shape[1:]
    rows = count * seq
    blocks = hid_ref.shape[0] // seq
    my_ep = lax.axis_index("ep")
    own = lax.axis_index("tp") * count + my_ep
    total = jnp.zeros((rows, lanes), f32)
    dense = jnp.zeros((rows, lanes), f32)
    for k in range(blocks):
        for t in range(seq):
            at = k * rows + t * count
            h_ref[at : at + count, :] = hid_ref[k * seq + t].astype(f32)
        h = h_ref[k * rows : (k + 1) * rows, :]
        total += h * h
        x = (h * gain_ref[k : k + 1, :]).astype(bf16)
        x_ref[:, k * lanes : (k + 1) * lanes] = x
        dense += x.astype(f32) * dgate_ref[k : k + 1, :]
    scale = lax.rsqrt(jnp.sum(total, axis=1, keepdims=True) / (blocks * lanes) + norm_eps)
    own_ref[...] = h_ref[pl.ds(own, blocks, stride=rows), :]
    dense_weight = jax.nn.sigmoid(jnp.sum(dense, axis=1, keepdims=True) * scale)

    tail = tail_ref[...]
    lane = lax.broadcasted_iota(jnp.int32, tail.shape, 1)
    scored = (lane >= top) & (lane < 2 * top)
    peak = jnp.max(jnp.where(scored, tail, -3e38), axis=1, keepdims=True)
    raised = jnp.where(scored, jnp.exp(jnp.minimum(tail - peak, 0.0)), 0.0)
    hits = (lane < top) & (tail.astype(jnp.int32) == my_ep)
    picked = jnp.where(hits, pltpu.roll(raised, lanes - top, 1), 0.0)
    row_weight = jnp.sum(picked, axis=1, keepdims=True) / jnp.sum(raised, axis=1, keepdims=True)

    x = x_ref[...]
    gate = jnp.dot(x, gate_ref[...], preferred_element_type=f32)
    up = jnp.dot(x, up_ref[...], preferred_element_type=f32)
    act = (clamped_unit(gate * scale, up * scale) * row_weight).astype(bf16)
    inner = jnp.dot(x, dup_ref[...], preferred_element_type=f32) * scale
    dact = (inner * jax.nn.sigmoid(inner) * dense_weight).astype(bf16)
    copies = new_states(
        state_ref,
        conv_ref,
        inner_ref,
        pre_ref,
        vec_ref,
        old_ref,
        state_out_ref,
        conv_out_ref,
        new_ref,
        taps_ref,
        sems,
    )
    wide = 4
    for j in range(blocks // wide):
        cols = slice(j * wide * lanes, (j + 1) * wide * lanes)
        y = jnp.dot(act, down_ref[:, cols], preferred_element_type=f32) + jnp.dot(
            dact, ddown_ref[:, cols], preferred_element_type=f32
        )
        for i in range(wide):
            for t in range(seq):
                t_ref[pl.ds(t * blocks + j * wide + i, count, stride=seq * blocks), :] = y[
                    t * count : (t + 1) * count, i * lanes : (i + 1) * lanes
                ]
    for r in range(rows):
        out_ref[r] = t_ref[r * blocks : (r + 1) * blocks, :].astype(bf16)
    for copy in copies:
        copy.wait()


def call(kernel, outs, args, scratch, limit, anywhere=(), sems=0, work=None, outside=()):
    vmem = pl.BlockSpec(memory_space=pltpu.VMEM)
    hbm = pl.BlockSpec(memory_space=pltpu.HBM)
    args = [
        pltpu.with_memory_space_constraint(v, pltpu.HBM) if i in anywhere else v
        for i, v in enumerate(args)
    ]
    return pl.pallas_call(
        kernel,
        out_shape=tuple(jax.ShapeDtypeStruct(shape, kind) for shape, kind in outs),
        in_specs=[hbm if i in anywhere else vmem for i in range(len(args))],
        out_specs=tuple(hbm if i in outside else vmem for i in range(len(outs))),
        scratch_shapes=[pltpu.VMEM(shape, kind) for shape, kind in scratch]
        + ([pltpu.SemaphoreType.DMA((sems,))] if sems else []),
        cost_estimate=work and pl.CostEstimate(
            flops=work, bytes_accessed=2**20, transcendentals=0
        ),
        compiler_params=pltpu.CompilerParams(vmem_limit_bytes=limit * 2**20),
    )(*args)


def final_kernel(terms_ref, own_ref, out_ref):
    count, blocks, lanes = terms_ref.shape
    total = own_ref[...]
    for r in range(count):
        total += terms_ref[r].astype(f32)
    for k in range(blocks):
        out_ref[:, k * lanes : (k + 1) * lanes] = total[k : k + 1, :].astype(bf16)


def final_stage(terms, own):
    _, blocks, lanes = terms.shape
    vmem = pl.BlockSpec(memory_space=pltpu.VMEM)
    return pl.pallas_call(
        final_kernel,
        name="final_stage",
        out_shape=jax.ShapeDtypeStruct((1, blocks * lanes), bf16),
        in_specs=[vmem] * 2,
        out_specs=vmem,
        compiler_params=pltpu.CompilerParams(vmem_limit_bytes=4 * 2**20),
    )(terms, own)


def direct(
    tokens,
    head_state,
    conv_state,
    conv_proj_state,
    first_gain,
    gate_weight,
    inner_weight,
    write_weight,
    read_weight,
    step_weight,
    conv_kernel,
    conv_proj_kernel,
    step_bias,
    log_rate,
    skip_gain,
    group_gain,
    out_weight,
    second_gain,
    routes,
    route_logits,
    expert_gate,
    expert_up,
    expert_down,
    dense_up,
    dense_down,
    dense_gate,
):
    n_ep = lax.axis_size("ep")
    n_tp = lax.axis_size("tp")
    n_all = n_ep * n_tp
    seq, width = tokens.shape
    rows = seq * n_ep
    channels = gate_weight.shape[1]
    half = channels // LANES * seq
    heads = step_weight.shape[1]
    state_cols = write_weight.shape[1]
    top = routes.shape[1]

    raw = lax.all_to_all(tokens, "ep", split_axis=1, concat_axis=0, tiled=True)

    swap = [(i, (i + 1) % n_tp) for i in range(n_tp)]
    other_weight = lax.ppermute(out_weight, "tp", swap)

    operands = (
        tokens,
        first_gain.reshape(1, width),
        write_weight,
        read_weight,
        step_weight.T,
        conv_state.transpose(1, 0, 2),
        conv_proj_state,
        conv_kernel,
        conv_proj_kernel,
        step_bias.reshape(1, heads),
        log_rate.reshape(1, heads),
        skip_gain.reshape(1, heads),
        group_gain.reshape(1, channels),
        routes,
        route_logits,
        head_state,
    )
    (opened,) = call(open_kernel, (((8, LANES), f32),), (), (), 1, work=WORK)
    early, vectors, tail, proj_out = call(
        functools.partial(early_stage, len(operands)),
        (
            ((8, half, LANES), f32),
            ((2, seq, state_cols), f32),
            ((seq, LANES), f32),
            (conv_proj_state.shape, bf16),
        ),
        (*operands, opened),
        (((2 * seq, channels), f32), (head_state.shape, f32)),
        6,
        (len(operands) - 1,),
        1,
    )

    raw, other_weight = lax.optimization_barrier((raw, other_weight))
    terms, tok_block = call(
        project_kernel,
        (((n_ep, 2 * half + 8, LANES), bf16), ((rows, LANES), f32)),
        (raw, first_gain.reshape(n_ep, LANES), gate_weight, inner_weight, tail),
        (((rows, LANES), f32), ((n_ep * (2 * half + 8), LANES), f32)),
        6,
        work=WORK,
    )
    terms = lax.all_to_all(terms, "ep", split_axis=0, concat_axis=0, tiled=True)

    mixed, conv, inner, tails = call(
        functools.partial(mixer_kernel, seq),
        (
            ((n_all, half // seq, LANES), bf16),
            ((half, LANES), f32),
            ((half, LANES), f32),
            ((rows, LANES), f32),
        ),
        (terms, early),
        (((max(n_ep * 8, half), LANES), f32),),
        4,
        work=WORK,
    )
    mixed = lax.all_to_all(mixed, ("ep", "tp"), split_axis=0, concat_axis=0, tiled=True)

    (hidden,) = call(
        functools.partial(hidden_kernel, n_ep),
        (((n_all, n_ep, LANES), bf16),),
        (mixed, out_weight, other_weight, tok_block),
        (((n_all * half // seq, LANES), f32), ((n_ep, channels), bf16)),
        6,
        work=WORK,
    )
    hidden = lax.all_to_all(hidden, ("ep", "tp"), split_axis=0, concat_axis=0, tiled=True)

    old = conv_state.transpose(1, 0, 2)
    terms, own_row, state_out, conv_out = call(
        functools.partial(expert_kernel, top, seq),
        (
            ((rows, n_ep, LANES), bf16),
            ((n_ep, LANES), f32),
            (head_state.shape, f32),
            (old.shape, bf16),
        ),
        (
            hidden,
            tails,
            second_gain.reshape(n_ep, LANES),
            dense_gate.reshape(n_ep, LANES),
            expert_gate[0],
            expert_up[0],
            expert_down[0],
            dense_up,
            dense_down,
            head_state,
            conv,
            inner,
            early,
            vectors,
            old,
        ),
        (
            ((rows, width), bf16),
            ((rows * n_ep, LANES), f32),
            ((rows * n_ep, LANES), f32),
            (head_state.shape, f32),
            (old.shape, bf16),
        ),
        8,
        sems=seq + 1,
        outside=(2, 3),
    )
    terms = lax.all_to_all(terms, ("ep", "tp"), split_axis=0, concat_axis=0, tiled=True)
    conv_out = conv_out.transpose(1, 0, 2)
    layer_out = final_stage(terms, own_row)
    return (layer_out, state_out, conv_out, proj_out)


def local(
    tokens,
    head_state,
    conv_state,
    conv_proj_state,
    first_gain,
    gate_weight,
    inner_weight,
    write_weight,
    read_weight,
    step_weight,
    conv_kernel,
    conv_proj_kernel,
    step_bias,
    log_rate,
    skip_gain,
    group_gain,
    out_weight,
    second_gain,
    routes,
    route_logits,
    expert_gate,
    expert_up,
    expert_down,
    dense_up,
    dense_down,
    dense_gate,
):
    n_ep = lax.axis_size("ep")
    n_tp = lax.axis_size("tp")
    n_all = n_ep * n_tp
    my_ep = lax.axis_index("ep")
    my_tp = lax.axis_index("tp")
    seq, width = tokens.shape
    rows = seq * n_ep
    half = gate_weight.shape[1]
    block = gate_weight.shape[0]

    if block == LANES and n_all == rows and seq == n_tp and half % LANES == 0:
        return direct(
            tokens,
            head_state,
            conv_state,
            conv_proj_state,
            first_gain,
            gate_weight,
            inner_weight,
            write_weight,
            read_weight,
            step_weight,
            conv_kernel,
            conv_proj_kernel,
            step_bias,
            log_rate,
            skip_gain,
            group_gain,
            out_weight,
            second_gain,
            routes,
            route_logits,
            expert_gate,
            expert_up,
            expert_down,
            dense_up,
            dense_down,
            dense_gate,
        )

    raw_block = lax.all_to_all(tokens, "ep", split_axis=1, concat_axis=0, tiled=True)

    tok = tokens.astype(f32)
    scale = lax.rsqrt(jnp.mean(tok * tok, axis=-1, keepdims=True) + norm_eps)
    normed_in = (tok * scale * first_gain).astype(bf16)
    write_proj = jnp.dot(normed_in, write_weight, preferred_element_type=f32).astype(bf16)
    read_proj = jnp.dot(normed_in, read_weight, preferred_element_type=f32).astype(bf16)
    step_raw = jnp.dot(normed_in, step_weight, preferred_element_type=f32)

    swap = [(i, (i + 1) % n_tp) for i in range(n_tp)]
    other_weight = lax.ppermute(out_weight, "tp", swap)

    gain_block = lax.dynamic_slice_in_dim(first_gain, my_ep * block, block, 0)
    scaled = (raw_block.astype(f32) * gain_block).astype(bf16)
    terms = jnp.concatenate(
        [
            jnp.dot(scaled, gate_weight, preferred_element_type=f32).astype(bf16),
            jnp.dot(scaled, inner_weight, preferred_element_type=f32).astype(bf16),
        ],
        axis=1,
    ).reshape(n_ep, seq, 2 * half)
    terms = lax.all_to_all(terms, "ep", split_axis=0, concat_axis=0, tiled=True)
    both = jnp.sum(terms.astype(f32), axis=0) * scale
    gate_proj = both[:, :half].astype(bf16)
    inner_proj = both[:, half:].astype(bf16)

    mixer_rows, state_out, conv_out, conv_proj_out = state_step(
        inner_proj,
        gate_proj,
        write_proj,
        read_proj,
        step_raw,
        conv_state,
        conv_proj_state,
        conv_kernel,
        conv_proj_kernel,
        step_bias,
        log_rate,
        skip_gain,
        group_gain,
        head_state,
        GROUPS // n_tp,
    )

    top = routes.shape[1]
    tail = jnp.concatenate(
        [routes.astype(bf16), route_logits, jnp.zeros((seq, TAIL - 2 * top), bf16)], axis=1
    )
    packed = jnp.concatenate([mixer_rows, tail], axis=1)
    packed = jnp.broadcast_to(packed[None], (n_all, seq, half + TAIL))
    packed = lax.all_to_all(packed, ("ep", "tp"), split_axis=0, concat_axis=0, tiled=True)
    packed = packed.reshape(n_ep, n_tp, seq, half + TAIL)
    own_half = lax.dynamic_index_in_dim(packed, my_tp, 1, keepdims=False)
    other_half = lax.dynamic_index_in_dim(packed, n_tp - 1 - my_tp, 1, keepdims=False)
    own_half = own_half.reshape(rows, half + TAIL)
    other_half = other_half.reshape(rows, half + TAIL)
    all_routes = own_half[:, half : half + top]
    all_logits = own_half[:, half + top : half + 2 * top]
    mixed = jnp.dot(own_half[:, :half], out_weight, preferred_element_type=f32) + jnp.dot(
        other_half[:, :half], other_weight, preferred_element_type=f32
    )
    hidden_block = (raw_block.astype(f32) + mixed).astype(bf16)

    hidden = jnp.broadcast_to(hidden_block[None], (n_ep, rows, block))
    hidden = lax.all_to_all(hidden, "ep", split_axis=0, concat_axis=0, tiled=True)
    hidden = hidden.transpose(1, 0, 2).reshape(rows, width)

    hid = hidden.astype(f32)
    normed = hid * lax.rsqrt(jnp.mean(hid * hid, axis=-1, keepdims=True) + norm_eps) * second_gain
    normed_mid = normed.astype(bf16)

    route_gates = jax.nn.softmax(all_logits.astype(f32), axis=-1)
    row_weight = jnp.sum(
        jnp.where(all_routes.astype(jnp.int32) == my_ep, route_gates, 0.0), axis=1, keepdims=True
    )
    dense_weight = jax.nn.sigmoid(
        jnp.sum(normed_mid.astype(f32) * dense_gate, axis=-1, keepdims=True)
    )
    activated = clamped_unit(
        jnp.dot(normed_mid, expert_gate[0], preferred_element_type=f32),
        jnp.dot(normed_mid, expert_up[0], preferred_element_type=f32),
    ).astype(bf16)
    dense_inner = jax.nn.silu(
        jnp.dot(normed_mid, dense_up, preferred_element_type=f32)
    ).astype(bf16)
    total = (
        jnp.dot(activated, expert_down[0], preferred_element_type=f32) * row_weight
        + jnp.dot(dense_inner, dense_down, preferred_element_type=f32) * dense_weight
    ).astype(bf16)

    row_share = rows // n_all
    total = total.reshape(n_all, row_share, width)
    total = lax.all_to_all(total, ("ep", "tp"), split_axis=0, concat_axis=0, tiled=True)
    summed = jnp.sum(total.astype(f32), axis=0)
    own_rows = lax.dynamic_slice_in_dim(
        hidden, (my_ep * n_tp + my_tp) * row_share, row_share, 0
    )
    layer_out = (own_rows.astype(f32) + summed).astype(bf16)
    return (layer_out, state_out, conv_out, conv_proj_out)


def solution(mesh):
    placed = (
        P("ep", None),
        P("ep", "tp", None, None),
        P("ep", None, "tp"),
        P("ep", None, None, "tp"),
        P(),
        P("ep", "tp"),
        P("ep", "tp"),
        P(None, "tp"),
        P(None, "tp"),
        P(None, "tp"),
        P(None, "tp"),
        P(None, None, "tp"),
        P("tp"),
        P("tp"),
        P("tp"),
        P("tp"),
        P("tp", "ep"),
        P(),
        P("ep", None),
        P("ep", None),
        P("ep", None, "tp"),
        P("ep", None, "tp"),
        P("ep", "tp", None),
        P(None, ("ep", "tp")),
        P(("ep", "tp"), None),
        P(),
    )
    return jax.shard_map(
        local,
        mesh=mesh,
        in_specs=placed,
        out_specs=(
            P(("ep", "tp"), None),
            P("ep", "tp", None, None),
            P("ep", None, "tp"),
            P("ep", None, None, "tp"),
        ),
        check_vma=False,
    )
```
